32 devices in a mesh: grp: 2 (over x), ep: 16 (over z, y, core).
Axes of the slice: x: 2, y: 2, z: 4, core: 2. Of those that a mesh axis runs over, the one named last changes fastest.
Arguments:
- tokens: bfloat16 [128, 2048], P(('grp', 'ep')), parts along dimension 0, may hold values from -6 to 6
- lengths: int32 [128], P(('grp', 'ep')), parts along dimension 0, may hold values from 128 to 1024, as said below
- cache_key: bfloat16 [128, 1024, 256], P(('grp', 'ep')), parts along dimension 0, may hold values from -6 to 6
- cache_value: bfloat16 [128, 1024, 256], P(('grp', 'ep')), parts along dimension 0, may hold values from -6 to 6
- routes: int32 [128, 2], P(('grp', 'ep')), parts along dimension 0, may hold values from 0 to 3, all different within a row
- route_logits: float32 [128, 2], P(('grp', 'ep')), parts along dimension 0, may hold values from -6 to 6
- mix_gain: float32 [2048], replicated, may hold values from 0.1 to 1.9
- query_gain: float32 [64], replicated, may hold values from 0.1 to 1.9
- key_gain: float32 [64], replicated, may hold values from 0.1 to 1.9
- head_bias: float32 [16], replicated, may hold values from -9 to -3.5
- w_query: bfloat16 [2048, 1024], P('ep'), may hold values from -0.125 to 0.125
- w_key: bfloat16 [2048, 256], P('ep'), may hold values from -0.125 to 0.125
- w_value: bfloat16 [2048, 256], P('ep'), may hold values from -0.125 to 0.125
- w_out: bfloat16 [1024, 2048], P(None, 'ep'), may hold values from -0.1875 to 0.1875
- ffn_gain: float32 [2048], replicated, may hold values from 0.1 to 1.9
- w_gate: bfloat16 [2048, 28672], P(None, 'ep'), may hold values from -0.125 to 0.125
- w_up: bfloat16 [2048, 28672], P(None, 'ep'), may hold values from -0.125 to 0.125
- w_down: bfloat16 [28672, 2048], P('ep'), may hold values from -0.0625 to 0.0625
Outputs:
- output: bfloat16 [128, 2048], P(('grp', 'ep')), parts along dimension 0
- new_key: bfloat16 [128, 256], P(('grp', 'ep')), parts along dimension 0
- new_value: bfloat16 [128, 256], P(('grp', 'ep')), parts along dimension 0
The draws below stay inside these ranges and needn't reach their ends.
There are 2 independent parts, one for each index of `grp`. The reference program is written for one: setup_inputs(seed, part) draws one part's arguments, and reference() takes and returns one part's arrays. A program takes and returns all parts, laid end to end along the dimension named above; an argument that names none is the same for every part. Nothing has to cross between parts.
Inputs may be any that keep to these rules, and one draw needn't show every extreme that they name: `lengths`: some sequence has all 1024 positions live.
All inputs are finite; a program needn't handle non-finite values.
Results may differ from the reference program's by a relative error of at most 0.0085.
Values may be sent and summed in bfloat16 or wider, within the bound.
A program may use at most 128 MiB of HBM per device.

```python
import jax
import jax.numpy as jnp
from jax import lax

D = 2048
HEADS = 16
KV_HEADS = 4
HEAD_DIM = 64
FF = 7168
EXPERTS = 4
TOP = 2
CACHE_LEN = 1024
BATCH = 64


def draw_lengths(key, part):
    spread = jax.random.randint(key, (BATCH,), CACHE_LEN // 8, CACHE_LEN + 1)
    chosen = jax.random.randint(jax.random.fold_in(key, 7), (), 0, BATCH)
    return jnp.where(jnp.arange(BATCH) == chosen, CACHE_LEN, spread).astype(jnp.int32)


def draw_head_bias(key, part):
    picker = jax.random.uniform(jax.random.fold_in(key, 1), (HEADS,), jnp.float32)
    quick = jax.random.uniform(jax.random.fold_in(key, 2), (HEADS,), jnp.float32, -4.5, -3.5)
    steady = jax.random.uniform(jax.random.fold_in(key, 3), (HEADS,), jnp.float32, -9.0, -7.5)
    portion = 0.5
    return jnp.where(picker < portion, quick, steady).astype(jnp.float32)


def steps_of(rng, dims, split, low, top_value):
    level, own = 1.0, jax.random.fold_in(rng, 6)
    for dim, parts in split:
        steps = jnp.exp(jax.random.uniform(jax.random.fold_in(own, dim), (parts,), jnp.float32, low / len(split), top_value / len(split)))
        level = level * jnp.repeat(steps, dims[dim] // parts).reshape([-1 if axis == dim else 1 for axis in range(len(dims))])
    return level


def distinct(key, rows, number_of, top, lift):
    ranking = jax.random.permutation(jax.random.fold_in(key, 1), number_of)
    favour = ranking
    for power in range(3):
        favour = favour * favour // number_of
    favour = favour * lift // number_of
    tickets = jax.random.randint(jax.random.fold_in(key, 2), (rows, number_of), 0, 4096) + favour
    fixed_rows = jax.random.permutation(jax.random.fold_in(key, 3), rows)[jnp.arange(number_of) % rows]
    tickets = jnp.where(jnp.arange(rows)[:, None] == fixed_rows[None, :], 1 << 14, tickets)
    priority = tickets * number_of + jnp.arange(number_of)
    return lax.top_k(priority.astype(jnp.int32), top)[1].astype(jnp.int32)


def normal_values(rng, dims, scale, bound, cuts=(), held_as=jnp.bfloat16):
    entries = scale * jax.random.normal(rng, dims, jnp.float32)
    if cuts:
        entries = entries * steps_of(rng, dims, cuts, -0.22, 0.18)
    return jnp.clip(entries, -bound, bound).astype(held_as)


def setup_inputs(seed: int = 0, part: int = 0) -> dict:
    arg_keys = jax.random.split(jax.random.key(seed), 19)
    part_keys = jax.random.split(jax.random.fold_in(arg_keys[18], part), 19)
    return {
        "tokens": normal_values(part_keys[0], (BATCH, D), 1.0, 6.0, ((0, 16),)),
        "lengths": draw_lengths(jax.random.fold_in(jax.random.fold_in(arg_keys[18], part), 71), part),
        "cache_key": normal_values(part_keys[2], (BATCH, CACHE_LEN, KV_HEADS * HEAD_DIM), 1.0, 6.0, ((0, 16),)),
        "cache_value": normal_values(part_keys[3], (BATCH, CACHE_LEN, KV_HEADS * HEAD_DIM), 1.0, 6.0, ((0, 16),)),
        "routes": distinct(part_keys[4], BATCH, EXPERTS, TOP, 4096),
        "route_logits": normal_values(part_keys[5], (BATCH, TOP), 1.5, 6.0, ((0, 16),), jnp.float32),
        "mix_gain": jnp.clip(1.0 + 0.18 * jax.random.normal(arg_keys[6], (D,), jnp.float32), 0.1, 1.9),
        "query_gain": jnp.clip(1.0 + 0.18 * jax.random.normal(arg_keys[7], (HEAD_DIM,), jnp.float32), 0.1, 1.9),
        "key_gain": jnp.clip(1.0 + 0.18 * jax.random.normal(arg_keys[8], (HEAD_DIM,), jnp.float32), 0.1, 1.9),
        "head_bias": draw_head_bias(jax.random.fold_in(arg_keys[18], 71), part),
        "w_query": normal_values(arg_keys[10], (D, HEADS * HEAD_DIM), D ** -0.5, 0.125, ((0, 16),)),
        "w_key": normal_values(arg_keys[11], (D, KV_HEADS * HEAD_DIM), D ** -0.5, 0.125, ((0, 16),)),
        "w_value": normal_values(arg_keys[12], (D, KV_HEADS * HEAD_DIM), D ** -0.5, 0.125, ((0, 16),)),
        "w_out": normal_values(arg_keys[13], (HEADS * HEAD_DIM, D), (HEADS * HEAD_DIM) ** -0.5, 0.1875, ((1, 16),)),
        "ffn_gain": jnp.clip(1.0 + 0.18 * jax.random.normal(arg_keys[14], (D,), jnp.float32), 0.1, 1.9),
        "w_gate": normal_values(arg_keys[15], (D, EXPERTS * FF), D ** -0.5, 0.125, ((1, 16),)),
        "w_up": normal_values(arg_keys[16], (D, EXPERTS * FF), D ** -0.5, 0.125, ((1, 16),)),
        "w_down": normal_values(arg_keys[17], (EXPERTS * FF, D), FF ** -0.5, 0.0625, ((0, 16),)),
    }


EPSILON = 1e-06

def rms_scaled(values, gain):
    return values * lax.rsqrt(lax.optimization_barrier(jnp.mean(values * values, axis=-1, keepdims=True)) + EPSILON) * gain

def route_weights(routes, route_logits):
    experts_iota = jnp.arange(EXPERTS, dtype=jnp.int32)[None, :]
    first_share = jax.nn.sigmoid(route_logits[:, 0:1] - route_logits[:, 1:2])
    second_share = jax.nn.sigmoid(route_logits[:, 1:2] - route_logits[:, 0:1])
    return jnp.where(routes[:, 0:1] == experts_iota, first_share, 0.0) + jnp.where(routes[:, 1:2] == experts_iota, second_share, 0.0)

def reference(tokens, lengths, cache_key, cache_value, routes, route_logits, mix_gain, query_gain, key_gain, head_bias, w_query, w_key, w_value, w_out, ffn_gain, w_gate, w_up, w_down):
    as_float = tokens.astype(jnp.float32)
    normed = rms_scaled(as_float, mix_gain).astype(jnp.bfloat16)
    queries = jnp.dot(normed, w_query, preferred_element_type=jnp.float32)
    fresh_key = jnp.dot(normed, w_key, preferred_element_type=jnp.float32)
    fresh_value = jnp.dot(normed, w_value, preferred_element_type=jnp.float32)
    batch_rows = tokens.shape[0]
    group_size = HEADS // KV_HEADS
    normed_query = rms_scaled(queries.reshape(batch_rows, HEADS, HEAD_DIM), query_gain).astype(jnp.bfloat16)
    normed_query = normed_query.reshape(batch_rows, KV_HEADS, group_size, HEAD_DIM)
    new_key = rms_scaled(fresh_key.reshape(batch_rows, KV_HEADS, HEAD_DIM), key_gain)
    new_key = new_key.reshape(batch_rows, KV_HEADS * HEAD_DIM).astype(jnp.bfloat16)
    new_value = fresh_value.astype(jnp.bfloat16)
    key_heads = cache_key.reshape(batch_rows, CACHE_LEN, KV_HEADS, HEAD_DIM).astype(jnp.float32)
    value_heads = cache_value.reshape(batch_rows, CACHE_LEN, KV_HEADS, HEAD_DIM).astype(jnp.float32)
    scores = jnp.einsum('bkgd,blkd->bkgl', normed_query.astype(jnp.float32), key_heads) * HEAD_DIM ** (-0.5)
    scores = scores + head_bias.reshape(KV_HEADS, group_size)[None, :, :, None]
    live_mask = jnp.arange(CACHE_LEN, dtype=jnp.int32)[None, None, None, :] < lengths.astype(jnp.int32)[:, None, None, None]
    remain = jnp.where(live_mask, jax.nn.log_sigmoid(-scores), 0.0)
    after_sum = lax.cumsum(remain, axis=3, reverse=True) - remain
    weights = jnp.where(live_mask, jnp.exp(jax.nn.log_sigmoid(scores) + after_sum), 0.0).astype(jnp.bfloat16)
    attended = jnp.einsum('bkgl,blkd->bkgd', weights.astype(jnp.float32), value_heads)
    attended = attended.reshape(batch_rows, HEADS * HEAD_DIM).astype(jnp.bfloat16)
    mixed = as_float + jnp.dot(attended, w_out, preferred_element_type=jnp.float32)
    expert_in = rms_scaled(mixed, ffn_gain).astype(jnp.bfloat16)
    gate_table = route_weights(routes, route_logits)
    expert_sum = jnp.zeros_like(mixed)
    for expert in range(EXPERTS):
        gate_value = jnp.dot(expert_in, w_gate[:, expert * FF:(expert + 1) * FF], preferred_element_type=jnp.float32)
        up_value = jnp.dot(expert_in, w_up[:, expert * FF:(expert + 1) * FF], preferred_element_type=jnp.float32)
        hidden = (jax.nn.silu(gate_value) * up_value * gate_table[:, expert:expert + 1]).astype(jnp.bfloat16)
        expert_sum = expert_sum + jnp.dot(hidden, w_down[expert * FF:(expert + 1) * FF], preferred_element_type=jnp.float32)
    return ((mixed + expert_sum).astype(jnp.bfloat16), new_key, new_value)
```

```python
import functools

import jax
import jax.numpy as jnp
from jax import lax
from jax.experimental import pallas as pl
from jax.experimental.pallas import tpu as pltpu
from jax.sharding import PartitionSpec as P

HEADS = 16
KV_HEADS = 4
HEAD_DIM = 64
FF = 7168
EXPERTS = 4


EPSILON = 1e-06


def rms_scaled(values, gain):
    return values * lax.rsqrt(jnp.mean(values * values, axis=-1, keepdims=True) + EPSILON) * gain


def route_weights(routes, route_logits):
    experts_iota = jnp.arange(EXPERTS, dtype=jnp.int32)[None, :]
    first_share = jax.nn.sigmoid(route_logits[:, 0:1] - route_logits[:, 1:2])
    second_share = jax.nn.sigmoid(route_logits[:, 1:2] - route_logits[:, 0:1])
    return jnp.where(routes[:, 0:1] == experts_iota, first_share, 0.0) + jnp.where(
        routes[:, 1:2] == experts_iota, second_share, 0.0
    )


def stick_attend(queries, lengths, cache_key, cache_value, query_gain, head_bias):
    batch_rows = queries.shape[0]
    cache_len = cache_key.shape[1]
    group_size = HEADS // KV_HEADS
    normed_query = rms_scaled(queries.reshape(batch_rows, HEADS, HEAD_DIM), query_gain).astype(
        jnp.bfloat16
    )
    normed_query = normed_query.reshape(batch_rows, KV_HEADS, group_size, HEAD_DIM)
    key_heads = cache_key.reshape(batch_rows, cache_len, KV_HEADS, HEAD_DIM)
    value_heads = cache_value.reshape(batch_rows, cache_len, KV_HEADS, HEAD_DIM)
    scores = jnp.einsum(
        "bkgd,blkd->bkgl", normed_query, key_heads, preferred_element_type=jnp.float32
    ) * HEAD_DIM ** (-0.5)
    scores = scores + head_bias.reshape(KV_HEADS, group_size)[None, :, :, None]
    live_mask = (
        jnp.arange(cache_len, dtype=jnp.int32)[None, None, None, :] < lengths[:, None, None, None]
    )
    remain = jnp.where(live_mask, jax.nn.log_sigmoid(-scores), 0.0)
    after_sum = lax.cumsum(remain, axis=3, reverse=True) - remain
    weights = jnp.where(live_mask, jnp.exp(jax.nn.log_sigmoid(scores) + after_sum), 0.0).astype(
        jnp.bfloat16
    )
    attended = jnp.einsum(
        "bkgl,blkd->bkgd", weights, value_heads, preferred_element_type=jnp.float32
    )
    return attended.reshape(batch_rows, HEADS * HEAD_DIM).astype(jnp.bfloat16)


def plain(
    tokens,
    lengths,
    cache_key,
    cache_value,
    routes,
    route_logits,
    mix_gain,
    query_gain,
    key_gain,
    head_bias,
    w_query,
    w_key,
    w_value,
    w_out,
    ffn_gain,
    w_gate,
    w_up,
    w_down,
):
    token_rows = tokens.shape[0]
    key_width = w_key.shape[1]
    as_float = tokens.astype(jnp.float32)
    normed = rms_scaled(as_float, mix_gain).astype(jnp.bfloat16)
    pieces = (
        lax.all_gather(w_query, "ep", axis=0, tiled=True),
        lax.all_gather(w_key, "ep", axis=0, tiled=True),
        lax.all_gather(w_value, "ep", axis=0, tiled=True),
    )
    queries, fresh_key, fresh_value = tuple(
        (jnp.dot(normed, weight, preferred_element_type=jnp.float32) for weight in pieces)
    )
    new_key = rms_scaled(fresh_key.reshape(token_rows, KV_HEADS, HEAD_DIM), key_gain)
    new_key = new_key.reshape(token_rows, key_width).astype(jnp.bfloat16)
    new_value = fresh_value.astype(jnp.bfloat16)
    attended = stick_attend(queries, lengths, cache_key, cache_value, query_gain, head_bias)
    mixed = as_float + jnp.dot(
        attended,
        lax.all_gather(w_out, "ep", axis=1, tiled=True),
        preferred_element_type=jnp.float32,
    )
    expert_in = rms_scaled(mixed, ffn_gain).astype(jnp.bfloat16)
    every_gate = lax.all_gather(route_weights(routes, route_logits), "ep", axis=0, tiled=True)
    ff_share = w_gate.shape[1]
    my_expert = lax.axis_index("ep") // (FF // ff_share)
    my_gate = lax.dynamic_slice_in_dim(every_gate, my_expert, 1, 1)
    input_rows = lax.all_gather(expert_in, "ep", axis=0, tiled=True)
    gate_value = jnp.dot(input_rows, w_gate, preferred_element_type=jnp.float32)
    up_value = jnp.dot(input_rows, w_up, preferred_element_type=jnp.float32)
    hidden = (jax.nn.silu(gate_value) * up_value * my_gate).astype(jnp.bfloat16)
    expert_sum = lax.psum_scatter(
        jnp.dot(hidden, w_down, preferred_element_type=jnp.float32),
        "ep",
        scatter_dimension=0,
        tiled=True,
    )
    return ((mixed + expert_sum).astype(jnp.bfloat16), new_key, new_value)


WEIGHT_PARTS = 2
DOWN_PARTS = 4
COLUMNS = 256


def dot(left, right):
    return jnp.dot(left, right, preferred_element_type=jnp.float32)


def iota(shape, dim):
    return lax.broadcasted_iota(jnp.int32, shape, dim)


def column(row):
    square = (row.shape[1], row.shape[1])
    return jnp.sum(
        jnp.where(iota(square, 0) == iota(square, 1), jnp.broadcast_to(row, square), 0.0),
        axis=1,
        keepdims=True,
    )


def finish(*refs):
    half = len(refs) // 2
    copies = [
        pltpu.make_async_copy(refs[i], refs[half + i], refs[-1].at[i]) for i in range(half)
    ]
    for copy in copies:
        copy.start()
    for copy in copies:
        copy.wait()


def fused(
    n,
    tokens_hbm,
    lengths_hbm,
    ck_hbm,
    cv_hbm,
    routes_hbm,
    logits_hbm,
    mix_gain_hbm,
    query_gain_hbm,
    key_gain_hbm,
    head_bias_hbm,
    wq_hbm,
    wk_hbm,
    wv_hbm,
    wo_hbm,
    ffn_gain_hbm,
    wg_hbm,
    wu_hbm,
    wd_hbm,
    out_any,
    new_key_any,
    new_value_any,
    tokens_ref,
    lengths_ref,
    routes_ref,
    logits_ref,
    mix_gain_ref,
    query_gain_ref,
    key_gain_ref,
    head_bias_ref,
    ffn_gain_ref,
    out_ref,
    new_key_ref,
    new_value_ref,
    wqkv,
    wo,
    ck,
    cv,
    wg,
    wu,
    wd,
    s1,
    r1,
    s2,
    r2,
    r3,
    r4,
    s5,
    p5,
    own5,
    t5,
    r5,
    gates_all,
    token_cols,
    aux_rows,
    attended_rows,
    own_mixed,
    gate_acc,
    up_acc,
    hidden,
    operand_sem,
    result_sem,
    small_sem,
    cache_sem,
    weight_sem,
    send_sem,
    recv_sem,
    direct_sem,
    relay_sem,
    pair_sem,
    spread_sem,
    twin_sem,
):
    me = lax.axis_index("ep")
    core, chip = me % 2, me // 2
    chips = n // 2
    sibling = me + 1 - 2 * core
    rows, width = tokens_ref.shape
    half_rows = rows * chips
    all_rows = rows * n
    share = width // n
    chip_share = width // chips
    q_width, k_width = wq_hbm.shape[1], wk_hbm.shape[1]
    cache_len = ck.shape[1]
    group_size = HEADS // KV_HEADS
    ff_share = wg.shape[1]
    my_expert = me // (FF // ff_share)

    barrier = pltpu.get_barrier_semaphore()
    chip_at = [chip]
    for k in range(1, chips):
        bit = k.bit_length() - 1
        flip = 2**bit * (1 - 2 * ((chip // 2**bit) % 2))
        chip_at.append(chip_at[k - 2**bit] + flip)
    peer_at = [2 * c + core for c in chip_at]
    furthest_first = range(chips - 1, 0, -1)
    for device in [peer_at[k] for k in furthest_first] + [sibling]:
        pl.semaphore_signal(
            barrier,
            inc=1,
            device_id={"ep": device},
            device_id_type=pl.DeviceIdType.MESH,
        )

    operands = [
        pltpu.make_async_copy(a, b, operand_sem.at[i])
        for i, (a, b) in enumerate(
            (
                (tokens_hbm, tokens_ref),
                (routes_hbm, routes_ref),
                (logits_hbm, logits_ref),
                (mix_gain_hbm, mix_gain_ref),
                (query_gain_hbm, query_gain_ref),
                (key_gain_hbm, key_gain_ref),
                (head_bias_hbm, head_bias_ref),
                (ffn_gain_hbm, ffn_gain_ref),
                (lengths_hbm, lengths_ref),
            )
        )
    ]
    for c in operands:
        c.start()

    my_rows = pl.ds(pl.multiple_of(core * share, share), share)
    small = [
        pltpu.make_async_copy(a, b, small_sem.at[i])
        for i, (a, b) in enumerate(
            (
                (wq_hbm, wqkv.at[my_rows, 0:q_width]),
                (wk_hbm, wqkv.at[my_rows, q_width : q_width + k_width]),
                (wv_hbm, wqkv.at[my_rows, q_width + k_width :]),
                (wo_hbm, wo.at[core]),
            )
        )
    ]
    for c in small:
        c.start()
    caches = [pltpu.make_async_copy(ck_hbm.at[b], ck.at[b], cache_sem.at[0]) for b in range(rows)]
    caches += [pltpu.make_async_copy(cv_hbm.at[b], cv.at[b], cache_sem.at[1]) for b in range(rows)]
    weights = []
    for which, (a, b) in enumerate(((wg_hbm, wg), (wu_hbm, wu), (wd_hbm, wd))):
        step = b.shape[0] // WEIGHT_PARTS
        for part in range(WEIGHT_PARTS):
            piece = pl.ds(part * step, step)
            weights.append(pltpu.make_async_copy(a.at[piece], b.at[piece], weight_sem.at[which]))

    results = [
        pltpu.make_async_copy(a, b, result_sem.at[i])
        for i, (a, b) in enumerate(
            ((out_ref, out_any), (new_key_ref, new_key_any), (new_value_ref, new_value_any))
        )
    ]
    for c in operands:
        c.wait()

    def send(stage, device, source, target, arrival):
        pltpu.make_async_remote_copy(
            src_ref=source,
            dst_ref=target,
            send_sem=send_sem.at[stage],
            recv_sem=arrival,
            device_id={"ep": device},
            device_id_type=pl.DeviceIdType.MESH,
        ).start()

    def arrived(sem, blocks):
        pltpu.make_async_copy(blocks, blocks, sem).wait()

    others = pl.ds(0, chips - 1)

    as_float = tokens_ref[...].astype(jnp.float32)
    scale = lax.rsqrt(jnp.mean(as_float * as_float, axis=1, keepdims=True) + EPSILON)
    lane = iota((rows, 128), 1)
    logit_gap = column(logits_ref[0:1] - logits_ref[1:2])
    chosen = [column(routes_ref[i : i + 1].astype(jnp.float32)) for i in range(2)]
    first_share = 1.0 / (1.0 + jnp.exp(-logit_gap))
    second_share = 1.0 / (1.0 + jnp.exp(logit_gap))
    expert_lane = (lane % EXPERTS).astype(jnp.float32)
    gates = jnp.where(chosen[0] == expert_lane, first_share, 0.0) + jnp.where(
        chosen[1] == expert_lane, second_share, 0.0
    )
    aux = jnp.where(lane < 3 * EXPERTS, gates, scale)
    high = aux.astype(jnp.bfloat16).astype(jnp.float32)
    middle = (aux - high).astype(jnp.bfloat16).astype(jnp.float32)
    low = aux - high - middle
    term = jnp.where(lane < 3 * EXPERTS, lane // EXPERTS, lane - 3 * EXPERTS)
    aux = jnp.where(term == 0, high, jnp.where(term == 1, middle, low))
    aux = jnp.concatenate([aux] * (chip_share // 128), axis=1)
    for p in range(chips):
        s1[p] = jnp.concatenate(
            [as_float[:, p * chip_share : (p + 1) * chip_share], aux], axis=0
        ).astype(jnp.bfloat16)
    pl.semaphore_wait(barrier, chips)
    for k in furthest_first:
        send(0, peer_at[k], s1.at[chip_at[k]], r1.at[chip], recv_sem.at[0])
    for c in small[:3]:
        c.wait()
    send(4, sibling, wqkv.at[my_rows], wqkv.at[my_rows], twin_sem.at[0])
    small[3].wait()
    send(5, sibling, wo.at[core], wo.at[core], twin_sem.at[1])
    for c in caches:
        c.start()
    r1[chip] = s1[chip]
    arrived(recv_sem.at[0], r1.at[others])
    for c in weights:
        c.start()
    for p in range(chips):
        block = r1[p].astype(jnp.float32)
        token_cols[p * rows : (p + 1) * rows, :] = block[:rows]
        aux_rows[p * rows : (p + 1) * rows, :] = block[rows:, :128]
    aux = aux_rows[...]
    lane = iota(aux.shape, 1)
    row_scale = jnp.sum(
        jnp.where((lane >= 3 * EXPERTS) & (lane < 3 * EXPERTS + 3), aux, 0.0), axis=1, keepdims=True
    )
    my_gain = mix_gain_ref[:, pl.ds(pl.multiple_of(chip * chip_share, chip_share), chip_share)]
    normed = (token_cols[...] * row_scale * my_gain).astype(jnp.bfloat16)
    arrived(twin_sem.at[0], wqkv.at[my_rows])

    partial = dot(normed, wqkv[...])
    for p in range(chips):
        s2[p] = partial[p * rows : (p + 1) * rows].astype(jnp.bfloat16)
    for k in furthest_first:
        send(1, peer_at[k], s2.at[chip_at[k]], r2.at[chip], recv_sem.at[1])
    r2[chip] = s2[chip]
    my_gate = jnp.sum(
        jnp.where((lane < 3 * EXPERTS) & (lane % EXPERTS == my_expert), aux, 0.0),
        axis=1,
        keepdims=True,
    )
    gates_all[core] = jnp.broadcast_to(my_gate, aux.shape)
    send(6, sibling, gates_all.at[core], gates_all.at[core], twin_sem.at[2])

    head_of_lane = iota((HEADS, q_width), 1) // HEAD_DIM
    own_lane = head_of_lane == iota((HEADS, q_width), 0)
    source_lane = iota((q_width, k_width), 0)
    target_lane = iota((q_width, k_width), 1)
    fold = jnp.where(
        (source_lane // (HEAD_DIM * group_size) == target_lane // HEAD_DIM)
        & (source_lane % HEAD_DIM == target_lane % HEAD_DIM),
        1.0,
        0.0,
    ).astype(jnp.bfloat16)
    later = jnp.where(
        iota((COLUMNS, COLUMNS), 0) > iota((COLUMNS, COLUMNS), 1), 1.0, 0.0
    ).astype(jnp.bfloat16)
    query_gain = jnp.concatenate([query_gain_ref[...]] * HEADS, axis=1)
    key_gain = jnp.concatenate([key_gain_ref[...]] * KV_HEADS, axis=1)
    blocks = cache_len // COLUMNS
    head_rows = rows * HEADS
    head_bias = jnp.concatenate([column(head_bias_ref[...])] * rows, axis=0)
    row_of = iota((head_rows, 1), 0) // HEADS
    lengths = jnp.zeros((head_rows, 1), jnp.int32)
    for b in range(rows):
        lengths = jnp.where(row_of == b, lengths_ref[:, b : b + 1], lengths)
    live = iota((head_rows, cache_len), 1) < lengths
    arrived(cache_sem.at[0], ck)
    arrived(cache_sem.at[1], cv)

    arrived(recv_sem.at[1], r2.at[others])
    total = r2[0].astype(jnp.float32)
    for p in range(1, chips):
        total = total + r2[p].astype(jnp.float32)
    queries = total[:, :q_width]
    spread = []
    for b in range(rows):
        wide = jnp.where(own_lane, jnp.broadcast_to(queries[b : b + 1], own_lane.shape), 0.0)
        mean = jnp.sum(wide * wide, axis=1, keepdims=True) / HEAD_DIM
        spread.append((wide * lax.rsqrt(mean + EPSILON) * query_gain).astype(jnp.bfloat16))
    folded = dot(jnp.concatenate(spread, axis=0), fold).astype(jnp.bfloat16)
    scores = jnp.concatenate(
        [
            lax.dot_general(
                folded[b * HEADS : (b + 1) * HEADS],
                ck[b],
                (((1,), (1,)), ((), ())),
                preferred_element_type=jnp.float32,
            )
            for b in range(rows)
        ],
        axis=0,
    )
    scores = scores * HEAD_DIM ** (-0.5) + head_bias
    tail_log = jnp.log1p(jnp.exp(-jnp.abs(scores)))
    remain = jnp.where(live, jnp.minimum(-scores, 0.0) - tail_log, 0.0)
    after = [None] * blocks
    carry = jnp.zeros((head_rows, 1), jnp.float32)
    for i in reversed(range(blocks)):
        block = remain[:, i * COLUMNS : (i + 1) * COLUMNS]
        high = block.astype(jnp.bfloat16)
        low = (block - high.astype(jnp.float32)).astype(jnp.bfloat16)
        after[i] = dot(high, later) + dot(low, later) + carry
        carry = carry + jnp.sum(block, axis=1, keepdims=True)
    after_sum = jnp.concatenate(after, axis=1)
    chance = jnp.exp(jnp.minimum(scores, 0.0) - tail_log + after_sum)
    weight = jnp.where(live, chance, 0.0).astype(jnp.bfloat16)
    mixed_heads = jnp.concatenate(
        [dot(weight[b * HEADS : (b + 1) * HEADS], cv[b]) for b in range(rows)], axis=0
    )
    own_group = (
        iota((head_rows, k_width), 1) // HEAD_DIM
        == iota((head_rows, k_width), 0) % HEADS // group_size
    )
    heads = jnp.where(own_group, mixed_heads, 0.0).astype(jnp.bfloat16)
    unfolded = lax.dot_general(
        heads,
        fold,
        (((1,), (1,)), ((), ())),
        preferred_element_type=jnp.float32,
    )
    attended = [
        jnp.sum(
            jnp.where(own_lane, unfolded[b * HEADS : (b + 1) * HEADS], 0.0), axis=0, keepdims=True
        )
        for b in range(rows)
    ]
    r3[chip] = jnp.concatenate(attended, axis=0).astype(jnp.bfloat16)

    for k in furthest_first:
        send(2, peer_at[k], r3.at[chip], r3.at[chip], recv_sem.at[2])

    fresh_key = total[:, q_width : q_width + k_width]
    new_value_ref[...] = total[:, q_width + k_width :].astype(jnp.bfloat16)
    squares = fresh_key * fresh_key
    key_lane = iota(squares.shape, 1) // HEAD_DIM
    key_scale = jnp.zeros_like(squares)
    for g in range(KV_HEADS):
        mean = jnp.sum(jnp.where(key_lane == g, squares, 0.0), axis=1, keepdims=True) / HEAD_DIM
        key_scale = jnp.where(key_lane == g, lax.rsqrt(mean + EPSILON), key_scale)
    new_key_ref[...] = (fresh_key * key_scale * key_gain).astype(jnp.bfloat16)
    for c in results[1:]:
        c.start()
    arrived(twin_sem.at[1], wo.at[core])
    arrived(twin_sem.at[2], gates_all.at[core])

    arrived(recv_sem.at[2], r3.at[others])
    for p in range(chips):
        attended_rows[p * rows : (p + 1) * rows, :] = r3[p].astype(jnp.float32)
    attended_all = attended_rows[...].astype(jnp.bfloat16)
    for h in range(2):
        columns = slice(h * share, (h + 1) * share)
        mixed = token_cols[:, columns] + dot(attended_all, wo[h])
        r4[chip, core, :, columns] = mixed.astype(jnp.bfloat16)

    mine = r4.at[chip, core]
    for k in furthest_first:
        send(3, peer_at[k], mine, mine, direct_sem.at[k])
    send(7, sibling, mine, mine, relay_sem.at[0])
    pick = jnp.where(
        iota((8, half_rows), 1) == iota((8, half_rows), 0) + chip * rows, 1.0, 0.0
    ).astype(jnp.bfloat16)
    squares = jnp.zeros((all_rows, chip_share), jnp.float32)
    gate_column = gates_all[...].reshape(all_rows, 128)[:, :1]
    for which, b in enumerate((wg, wu, wd)):
        arrived(weight_sem.at[which], b)

    def chunk(k, squares):
        source = chip_at[k]
        columns = pl.ds(pl.multiple_of(source * chip_share, chip_share), chip_share)
        arrived(relay_sem.at[k], r4.at[source, core])
        own_mixed[:, columns] = dot(pick, r4[source, core])[:rows]
        block = r4[source].reshape(all_rows, chip_share).astype(jnp.float32)
        squares = squares + block * block
        entry = (block * ffn_gain_ref[:, columns]).astype(jnp.bfloat16)
        if k == chips - 1:
            scale = lax.rsqrt(jnp.sum(squares, axis=1, keepdims=True) / width + EPSILON)
        for i in range(ff_share // COLUMNS):
            inner = slice(i * COLUMNS, (i + 1) * COLUMNS)
            gate_value = dot(entry, wg[columns, inner])
            up_value = dot(entry, wu[columns, inner])
            if k:
                gate_value = gate_value + gate_acc[:, inner]
                up_value = up_value + up_acc[:, inner]
            if k == chips - 1:
                gate_value = gate_value * scale
                silu = gate_value / (1.0 + jnp.exp(-gate_value))
                hidden[:, inner] = (silu * (up_value * scale) * gate_column).astype(jnp.bfloat16)
            else:
                gate_acc[:, inner] = gate_value
                up_acc[:, inner] = up_value
        return squares

    for k in range(1, chips):
        block = r4.at[chip_at[k], core]
        arrived(direct_sem.at[k], block)
        send(7, sibling, block, block, relay_sem.at[k])
        squares = chunk(k - 1, squares)
    squares = chunk(chips - 1, squares)

    step = width // DOWN_PARTS

    def spread_sums(part):
        arrived(pair_sem.at[part], p5.at[part])
        both = own5[part] + p5[part].astype(jnp.float32)
        for p in range(chips):
            t5[part, p] = both[p * rows : (p + 1) * rows].astype(jnp.bfloat16)
        for k in furthest_first:
            send(9, peer_at[k], t5.at[part, chip_at[k]], r5.at[part, chip], spread_sem.at[part])
        r5[part, chip] = t5[part, chip]

    for part in range(DOWN_PARTS):
        partial = dot(hidden[...], wd[:, part * step : (part + 1) * step])
        lower, upper = partial[:half_rows], partial[half_rows:]
        own5[part] = jnp.where(core == 0, lower, upper)
        s5[part] = jnp.where(core == 0, upper, lower).astype(jnp.bfloat16)
        send(8, sibling, s5.at[part], p5.at[part], pair_sem.at[part])
        if part > 1:
            spread_sums(part - 2)
    spread_sums(DOWN_PARTS - 2)
    spread_sums(DOWN_PARTS - 1)
    for part in range(DOWN_PARTS):
        arrived(spread_sem.at[part], r5.at[part, others])
        total = own_mixed[:, part * step : (part + 1) * step]
        for p in range(chips):
            total = total + r5[part, p].astype(jnp.float32)
        out_ref[:, part * step : (part + 1) * step] = total.astype(jnp.bfloat16)
    results[0].start()
    arrived(send_sem.at[0], s1.at[others])
    arrived(send_sem.at[1], s2.at[others])
    arrived(send_sem.at[2], r3.at[others])
    arrived(send_sem.at[3], r4.at[others, 0])
    arrived(send_sem.at[4], wqkv.at[my_rows])
    arrived(send_sem.at[5], wo.at[core])
    arrived(send_sem.at[6], gates_all.at[core])
    arrived(send_sem.at[7], r4.at[:, 0])
    arrived(send_sem.at[8], s5)
    arrived(send_sem.at[9], t5.at[:, others])
    for c in results:
        c.wait()


def local(
    n,
    tokens,
    lengths,
    cache_key,
    cache_value,
    routes,
    route_logits,
    mix_gain,
    query_gain,
    key_gain,
    head_bias,
    w_query,
    w_key,
    w_value,
    w_out,
    ffn_gain,
    w_gate,
    w_up,
    w_down,
):
    rows, width = tokens.shape
    chips = n // 2
    all_rows, half_rows = rows * n, rows * chips
    share, chip_share = width // n, width // chips
    q_width, k_width = w_query.shape[1], w_key.shape[1]
    wide = q_width + k_width + w_value.shape[1]
    step = width // DOWN_PARTS
    ff_share = w_gate.shape[1]
    anywhere = pl.BlockSpec(memory_space=pl.ANY)
    bf16, f32 = jnp.bfloat16, jnp.float32

    def like(array):
        return pltpu.VMEM(array.shape, array.dtype)

    flops = 2 * all_rows * 3 * w_gate.shape[0] * w_gate.shape[1]
    shapes = ((rows, width), (rows, k_width), (rows, w_value.shape[1]))
    results = pl.pallas_call(
        functools.partial(fused, n),
        out_shape=tuple(pltpu.VMEM(shape, bf16) for shape in shapes),
        in_specs=[anywhere] * 18,
        out_specs=(anywhere,) * 3,
        scratch_shapes=[
            like(tokens),
            pltpu.VMEM((1, rows), lengths.dtype),
            pltpu.VMEM(routes.shape[::-1], routes.dtype),
            pltpu.VMEM(route_logits.shape[::-1], f32),
            pltpu.VMEM((1, width), f32),
            pltpu.VMEM((1, HEAD_DIM), f32),
            pltpu.VMEM((1, HEAD_DIM), f32),
            pltpu.VMEM((1, HEADS), f32),
            pltpu.VMEM((1, width), f32),
            *(pltpu.VMEM(shape, bf16) for shape in shapes),
            pltpu.VMEM((chip_share, wide), bf16),
            pltpu.VMEM((2, *w_out.shape), bf16),
            like(cache_key),
            like(cache_value),
            like(w_gate),
            like(w_up),
            like(w_down),
            pltpu.VMEM((chips, 2 * rows, chip_share), bf16),
            pltpu.VMEM((chips, 2 * rows, chip_share), bf16),
            pltpu.VMEM((chips, rows, wide), bf16),
            pltpu.VMEM((chips, rows, wide), bf16),
            pltpu.VMEM((chips, rows, q_width), bf16),
            pltpu.VMEM((chips, 2, half_rows, chip_share), bf16),
            pltpu.VMEM((DOWN_PARTS, half_rows, step), bf16),
            pltpu.VMEM((DOWN_PARTS, half_rows, step), bf16),
            pltpu.VMEM((DOWN_PARTS, half_rows, step), f32),
            pltpu.VMEM((DOWN_PARTS, chips, rows, step), bf16),
            pltpu.VMEM((DOWN_PARTS, chips, rows, step), bf16),
            pltpu.VMEM((2, half_rows, 128), f32),
            pltpu.VMEM((half_rows, chip_share), f32),
            pltpu.VMEM((half_rows, 128), f32),
            pltpu.VMEM((half_rows, q_width), f32),
            pltpu.VMEM((rows, width), f32),
            pltpu.VMEM((all_rows, ff_share), f32),
            pltpu.VMEM((all_rows, ff_share), f32),
            pltpu.VMEM((all_rows, ff_share), bf16),
            pltpu.SemaphoreType.DMA((9,)),
            pltpu.SemaphoreType.DMA((3,)),
            pltpu.SemaphoreType.DMA((4,)),
            pltpu.SemaphoreType.DMA((2,)),
            pltpu.SemaphoreType.DMA((3,)),
            pltpu.SemaphoreType.DMA((10,)),
            pltpu.SemaphoreType.DMA((3,)),
            pltpu.SemaphoreType.DMA((chips,)),
            pltpu.SemaphoreType.DMA((chips,)),
            pltpu.SemaphoreType.DMA((DOWN_PARTS,)),
            pltpu.SemaphoreType.DMA((DOWN_PARTS,)),
            pltpu.SemaphoreType.DMA((3,)),
        ],
        compiler_params=pltpu.CompilerParams(
            collective_id=0, has_side_effects=True, vmem_limit_bytes=60 * 1024 * 1024
        ),
        cost_estimate=pl.CostEstimate(flops=flops, bytes_accessed=flops // all_rows, transcendentals=0),
    )(
        tokens,
        lengths.reshape(1, -1),
        cache_key,
        cache_value,
        routes.T,
        route_logits.T,
        mix_gain.reshape(1, -1),
        query_gain.reshape(1, -1),
        key_gain.reshape(1, -1),
        head_bias.reshape(1, -1),
        w_query,
        w_key,
        w_value,
        w_out,
        ffn_gain.reshape(1, -1),
        w_gate,
        w_up,
        w_down,
    )
    return pl.pallas_call(
        finish,
        out_shape=tuple(jax.ShapeDtypeStruct(shape, bf16) for shape in shapes),
        in_specs=[anywhere] * len(shapes),
        out_specs=(anywhere,) * len(shapes),
        scratch_shapes=[pltpu.SemaphoreType.DMA((len(shapes),))],
    )(*(pltpu.with_memory_space_constraint(result, pltpu.VMEM) for result in results))


def solution(mesh):
    n = mesh.shape["ep"]

    def body(*arrays):
        tokens, w_gate = arrays[0], arrays[15]
        share = tokens.shape[1] // n
        aligned = share == 128 and n & (n - 1) == 0 and n % 4 == 0
        halves = (FF // w_gate.shape[1]) % 2 == 0 and arrays[13].shape[1] == share
        if aligned and halves and w_gate.shape[1] % COLUMNS == 0 and tokens.shape[0] * n % 64 == 0:
            return local(n, *arrays)
        return plain(*arrays)

    return jax.shard_map(
        body,
        mesh=mesh,
        in_specs=(
            P(("grp", "ep"), None),
            P(("grp", "ep")),
            P(("grp", "ep"), None, None),
            P(("grp", "ep"), None, None),
            P(("grp", "ep"), None),
            P(("grp", "ep"), None),
            P(),
            P(),
            P(),
            P(),
            P("ep", None),
            P("ep", None),
            P("ep", None),
            P(None, "ep"),
            P(),
            P(None, "ep"),
            P(None, "ep"),
            P("ep", None),
        ),
        out_specs=(P(("grp", "ep"), None), P(("grp", "ep"), None), P(("grp", "ep"), None)),
        check_vma=False,
    )
```

```python
import functools

import jax
import jax.numpy as jnp
from jax import lax
from jax.experimental import pallas as pl
from jax.experimental.pallas import tpu as pltpu
from jax.sharding import PartitionSpec as P

HEADS = 16
KV_HEADS = 4
HEAD_DIM = 64
FF = 7168
EXPERTS = 4


EPSILON = 1e-06


def rms_scaled(values, gain):
    return values * lax.rsqrt(jnp.mean(values * values, axis=-1, keepdims=True) + EPSILON) * gain


def route_weights(routes, route_logits):
    experts_iota = jnp.arange(EXPERTS, dtype=jnp.int32)[None, :]
    first_share = jax.nn.sigmoid(route_logits[:, 0:1] - route_logits[:, 1:2])
    second_share = jax.nn.sigmoid(route_logits[:, 1:2] - route_logits[:, 0:1])
    return jnp.where(routes[:, 0:1] == experts_iota, first_share, 0.0) + jnp.where(
        routes[:, 1:2] == experts_iota, second_share, 0.0
    )


def stick_attend(queries, lengths, cache_key, cache_value, query_gain, head_bias):
    batch_rows = queries.shape[0]
    cache_len = cache_key.shape[1]
    group_size = HEADS // KV_HEADS
    normed_query = rms_scaled(queries.reshape(batch_rows, HEADS, HEAD_DIM), query_gain).astype(
        jnp.bfloat16
    )
    normed_query = normed_query.reshape(batch_rows, KV_HEADS, group_size, HEAD_DIM)
    key_heads = cache_key.reshape(batch_rows, cache_len, KV_HEADS, HEAD_DIM)
    value_heads = cache_value.reshape(batch_rows, cache_len, KV_HEADS, HEAD_DIM)
    scores = jnp.einsum(
        "bkgd,blkd->bkgl", normed_query, key_heads, preferred_element_type=jnp.float32
    ) * HEAD_DIM ** (-0.5)
    scores = scores + head_bias.reshape(KV_HEADS, group_size)[None, :, :, None]
    live_mask = (
        jnp.arange(cache_len, dtype=jnp.int32)[None, None, None, :] < lengths[:, None, None, None]
    )
    remain = jnp.where(live_mask, jax.nn.log_sigmoid(-scores), 0.0)
    after_sum = lax.cumsum(remain, axis=3, reverse=True) - remain
    weights = jnp.where(live_mask, jnp.exp(jax.nn.log_sigmoid(scores) + after_sum), 0.0).astype(
        jnp.bfloat16
    )
    attended = jnp.einsum(
        "bkgl,blkd->bkgd", weights, value_heads, preferred_element_type=jnp.float32
    )
    return attended.reshape(batch_rows, HEADS * HEAD_DIM).astype(jnp.bfloat16)


def plain(
    tokens,
    lengths,
    cache_key,
    cache_value,
    routes,
    route_logits,
    mix_gain,
    query_gain,
    key_gain,
    head_bias,
    w_query,
    w_key,
    w_value,
    w_out,
    ffn_gain,
    w_gate,
    w_up,
    w_down,
):
    token_rows = tokens.shape[0]
    key_width = w_key.shape[1]
    as_float = tokens.astype(jnp.float32)
    normed = rms_scaled(as_float, mix_gain).astype(jnp.bfloat16)
    pieces = (
        lax.all_gather(w_query, "ep", axis=0, tiled=True),
        lax.all_gather(w_key, "ep", axis=0, tiled=True),
        lax.all_gather(w_value, "ep", axis=0, tiled=True),
    )
    queries, fresh_key, fresh_value = tuple(
        (jnp.dot(normed, weight, preferred_element_type=jnp.float32) for weight in pieces)
    )
    new_key = rms_scaled(fresh_key.reshape(token_rows, KV_HEADS, HEAD_DIM), key_gain)
    new_key = new_key.reshape(token_rows, key_width).astype(jnp.bfloat16)
    new_value = fresh_value.astype(jnp.bfloat16)
    attended = stick_attend(queries, lengths, cache_key, cache_value, query_gain, head_bias)
    mixed = as_float + jnp.dot(
        attended,
        lax.all_gather(w_out, "ep", axis=1, tiled=True),
        preferred_element_type=jnp.float32,
    )
    expert_in = rms_scaled(mixed, ffn_gain).astype(jnp.bfloat16)
    every_gate = lax.all_gather(route_weights(routes, route_logits), "ep", axis=0, tiled=True)
    ff_share = w_gate.shape[1]
    my_expert = lax.axis_index("ep") // (FF // ff_share)
    my_gate = lax.dynamic_slice_in_dim(every_gate, my_expert, 1, 1)
    input_rows = lax.all_gather(expert_in, "ep", axis=0, tiled=True)
    gate_value = jnp.dot(input_rows, w_gate, preferred_element_type=jnp.float32)
    up_value = jnp.dot(input_rows, w_up, preferred_element_type=jnp.float32)
    hidden = (jax.nn.silu(gate_value) * up_value * my_gate).astype(jnp.bfloat16)
    expert_sum = lax.psum_scatter(
        jnp.dot(hidden, w_down, preferred_element_type=jnp.float32),
        "ep",
        scatter_dimension=0,
        tiled=True,
    )
    return ((mixed + expert_sum).astype(jnp.bfloat16), new_key, new_value)


WEIGHT_PARTS = 2
DOWN_PARTS = 4
SCHEDULE = (0, (0,), 1, 2, 3, 4, (1,), 5, (2,), 6, (3,), 7, (4,), (5, 6), (7,))
COLUMNS = 256


def dot(left, right):
    return jnp.dot(left, right, preferred_element_type=jnp.float32)


def iota(shape, dim):
    return lax.broadcasted_iota(jnp.int32, shape, dim)


def column(row):
    square = (row.shape[1], row.shape[1])
    return jnp.sum(
        jnp.where(iota(square, 0) == iota(square, 1), jnp.broadcast_to(row, square), 0.0),
        axis=1,
        keepdims=True,
    )


def finish(*refs):
    half = len(refs) // 2
    copies = [
        pltpu.make_async_copy(refs[i], refs[half + i], refs[-1].at[i]) for i in range(half)
    ]
    for copy in copies:
        copy.start()
    for copy in copies:
        copy.wait()


def fused(
    n,
    tokens_hbm,
    lengths_hbm,
    ck_hbm,
    cv_hbm,
    routes_hbm,
    logits_hbm,
    mix_gain_hbm,
    query_gain_hbm,
    key_gain_hbm,
    head_bias_hbm,
    wq_hbm,
    wk_hbm,
    wv_hbm,
    wo_hbm,
    ffn_gain_hbm,
    wg_hbm,
    wu_hbm,
    wd_hbm,
    out_any,
    new_key_any,
    new_value_any,
    tokens_ref,
    lengths_ref,
    routes_ref,
    logits_ref,
    mix_gain_ref,
    query_gain_ref,
    key_gain_ref,
    head_bias_ref,
    ffn_gain_ref,
    out_ref,
    new_key_ref,
    new_value_ref,
    wq_raw,
    wqkv,
    wo,
    ck,
    kt,
    cv,
    wg,
    wu,
    wd,
    s1,
    r1,
    s2,
    r2,
    s2kv,
    r2kv,
    s3,
    r3,
    r4,
    s5,
    p5,
    own5,
    t5,
    r5,
    gates_all,
    token_cols,
    aux_rows,
    attended_rows,
    own_mixed,
    gate_acc,
    up_acc,
    hidden,
    operand_sem,
    result_sem,
    small_sem,
    cache_sem,
    weight_sem,
    send_sem,
    recv_sem,
    direct_sem,
    relay_sem,
    pair_sem,
    spread_sem,
    twin_sem,
):
    me = lax.axis_index("ep")
    core, chip = me % 2, me // 2
    chips = n // 2
    other = 1 - core
    sibling = 2 * chip + other
    rows, width = tokens_ref.shape
    half_rows = rows * chips
    all_rows = rows * n
    share = width // n
    chip_share = width // chips
    q_width, k_width = wq_hbm.shape[1], wk_hbm.shape[1]
    cache_len = ck.shape[1]
    group_size = HEADS // KV_HEADS
    ff_share = wg.shape[1]
    my_expert = me // (FF // ff_share)

    barrier = pltpu.get_barrier_semaphore()
    chip_at = [chip]
    for k in range(1, chips):
        bit = k.bit_length() - 1
        flip = 2**bit * (1 - 2 * ((chip // 2**bit) % 2))
        chip_at.append(chip_at[k - 2**bit] + flip)
    peer_at = [2 * c + other for c in chip_at]
    furthest_first = range(chips - 1, -1, -1)
    for k in furthest_first:
        pl.semaphore_signal(
            barrier,
            inc=1,
            device_id={"ep": peer_at[k]},
            device_id_type=pl.DeviceIdType.MESH,
        )

    operands = [
        pltpu.make_async_copy(a, b, operand_sem.at[i])
        for i, (a, b) in enumerate(
            (
                (tokens_hbm, tokens_ref),
                (routes_hbm, routes_ref),
                (logits_hbm, logits_ref),
                (mix_gain_hbm, mix_gain_ref),
                (query_gain_hbm, query_gain_ref),
                (key_gain_hbm, key_gain_ref),
                (head_bias_hbm, head_bias_ref),
                (ffn_gain_hbm, ffn_gain_ref),
                (lengths_hbm, lengths_ref),
            )
        )
    ]
    for c in operands:
        c.start()

    my_rows = pl.ds(pl.multiple_of(core * share, share), share)
    small = [
        pltpu.make_async_copy(a, b, small_sem.at[i])
        for i, (a, b) in enumerate(
            (
                (wq_hbm, wq_raw),
                (wk_hbm, wqkv.at[my_rows, q_width : q_width + k_width]),
                (wv_hbm, wqkv.at[my_rows, q_width + k_width :]),
            )
        )
    ]
    for head in range(HEADS):
        place = head % group_size * KV_HEADS + head // group_size
        small.append(
            pltpu.make_async_copy(
                wo_hbm.at[head * HEAD_DIM : (head + 1) * HEAD_DIM],
                wo.at[core, place * HEAD_DIM : (place + 1) * HEAD_DIM],
                small_sem.at[3],
            )
        )
    for c in small:
        c.start()
    caches = [pltpu.make_async_copy(ck_hbm.at[b], ck.at[b], cache_sem.at[0]) for b in range(rows)]
    caches += [pltpu.make_async_copy(cv_hbm.at[b], cv.at[b], cache_sem.at[1]) for b in range(rows)]
    weights = []
    for which, (a, b) in enumerate(((wg_hbm, wg), (wu_hbm, wu), (wd_hbm, wd))):
        step = b.shape[0] // WEIGHT_PARTS
        for part in range(WEIGHT_PARTS):
            piece = pl.ds(part * step, step)
            weights.append(pltpu.make_async_copy(a.at[piece], b.at[piece], weight_sem.at[which]))

    results = [
        pltpu.make_async_copy(a, b, result_sem.at[i])
        for i, (a, b) in enumerate(
            ((out_ref, out_any), (new_key_ref, new_key_any), (new_value_ref, new_value_any))
        )
    ]
    for c in operands:
        c.wait()

    def send(stage, device, source, target, arrival):
        pltpu.make_async_remote_copy(
            src_ref=source,
            dst_ref=target,
            send_sem=send_sem.at[stage],
            recv_sem=arrival,
            device_id={"ep": device},
            device_id_type=pl.DeviceIdType.MESH,
        ).start()

    def arrived(sem, blocks):
        pltpu.make_async_copy(blocks, blocks, sem).wait()

    others = pl.ds(0, chips - 1)

    as_float = tokens_ref[...].astype(jnp.float32)
    scale = lax.rsqrt(jnp.mean(as_float * as_float, axis=1, keepdims=True) + EPSILON)
    lane = iota((rows, 128), 1)
    logit_gap = column(logits_ref[0:1] - logits_ref[1:2])
    chosen = [column(routes_ref[i : i + 1].astype(jnp.float32)) for i in range(2)]
    first_share = 1.0 / (1.0 + jnp.exp(-logit_gap))
    second_share = 1.0 / (1.0 + jnp.exp(logit_gap))
    expert_lane = (lane % EXPERTS).astype(jnp.float32)
    gates = jnp.where(chosen[0] == expert_lane, first_share, 0.0) + jnp.where(
        chosen[1] == expert_lane, second_share, 0.0
    )
    aux = jnp.where(lane < 3 * EXPERTS, gates, scale)
    high = aux.astype(jnp.bfloat16).astype(jnp.float32)
    middle = (aux - high).astype(jnp.bfloat16).astype(jnp.float32)
    low = aux - high - middle
    term = jnp.where(lane < 3 * EXPERTS, lane // EXPERTS, lane - 3 * EXPERTS)
    aux = jnp.where(term == 0, high, jnp.where(term == 1, middle, low))
    aux = jnp.concatenate([aux] * (chip_share // 128), axis=1)
    for p in range(chips):
        s1[p] = jnp.concatenate(
            [as_float[:, p * chip_share : (p + 1) * chip_share], aux], axis=0
        ).astype(jnp.bfloat16)
    for c in small[:3]:
        c.wait()
    left_half = iota((share, 2 * HEAD_DIM), 1) < HEAD_DIM
    for place in range(0, HEADS, 2):
        halves = []
        for side in range(2):
            head = (place + side) % KV_HEADS * group_size + (place + side) // KV_HEADS
            start = head // 2 * 2 * HEAD_DIM
            half = wq_raw[:, start : start + 2 * HEAD_DIM].astype(jnp.float32)
            halves.append(half if head % 2 == side else pltpu.roll(half, HEAD_DIM, 1))
        wqkv[my_rows, place * HEAD_DIM : (place + 2) * HEAD_DIM] = jnp.where(
            left_half, halves[0], halves[1]
        ).astype(jnp.bfloat16)
    pl.semaphore_wait(barrier, chips)
    for k in furthest_first:
        send(0, peer_at[k], s1.at[chip_at[k]], r1.at[chip], recv_sem.at[0])
    send(4, sibling, wqkv.at[my_rows], wqkv.at[my_rows], twin_sem.at[0])
    for c in caches:
        c.start()
    arrived(recv_sem.at[0], r1)
    for c in weights:
        c.start()
    for p in range(chips):
        block = r1[p].astype(jnp.float32)
        token_cols[p * rows : (p + 1) * rows, :] = block[:rows]
        aux_rows[p * rows : (p + 1) * rows, :] = block[rows:, :128]
    aux = aux_rows[...]
    lane = iota(aux.shape, 1)
    row_scale = jnp.sum(
        jnp.where((lane >= 3 * EXPERTS) & (lane < 3 * EXPERTS + 3), aux, 0.0), axis=1, keepdims=True
    )
    my_gain = mix_gain_ref[:, pl.ds(pl.multiple_of(chip * chip_share, chip_share), chip_share)]
    normed = (token_cols[...] * row_scale * my_gain).astype(jnp.bfloat16)
    arrived(twin_sem.at[0], wqkv.at[my_rows])

    partial = dot(normed, wqkv[:, :q_width])
    for p in range(chips):
        s2[p] = partial[p * rows : (p + 1) * rows].astype(jnp.bfloat16)
    for k in furthest_first:
        send(1, peer_at[k], s2.at[chip_at[k]], r2.at[chip], recv_sem.at[1])
    partial = dot(normed, wqkv[:, q_width:])
    for p in range(chips):
        s2kv[p] = partial[p * rows : (p + 1) * rows].astype(jnp.bfloat16)
    for k in furthest_first:
        send(10, peer_at[k], s2kv.at[chip_at[k]], r2kv.at[chip], recv_sem.at[3])
    arrived(small_sem.at[3], wo.at[core])
    send(5, sibling, wo.at[core], wo.at[core], twin_sem.at[1])
    my_gate = jnp.sum(
        jnp.where((lane < 3 * EXPERTS) & (lane % EXPERTS == my_expert), aux, 0.0),
        axis=1,
        keepdims=True,
    )
    gates_all[other] = jnp.broadcast_to(my_gate, aux.shape)
    send(6, sibling, gates_all.at[other], gates_all.at[other], twin_sem.at[2])

    own_group = iota((HEADS, k_width), 1) // HEAD_DIM == iota((HEADS, k_width), 0) % KV_HEADS
    later = jnp.where(
        iota((COLUMNS, COLUMNS), 0) > iota((COLUMNS, COLUMNS), 1), 1.0, 0.0
    ).astype(jnp.bfloat16)
    query_gain = jnp.concatenate([query_gain_ref[...]] * KV_HEADS, axis=1)
    key_gain = jnp.concatenate([key_gain_ref[...]] * KV_HEADS, axis=1)
    blocks = cache_len // COLUMNS
    head_rows = rows * HEADS
    place, head = iota((HEADS, HEADS), 0), iota((HEADS, HEADS), 1)
    head_bias = jnp.where(
        head == place % KV_HEADS * group_size + place // KV_HEADS,
        jnp.broadcast_to(head_bias_ref[...], head.shape),
        0.0,
    )
    head_bias = jnp.concatenate([jnp.sum(head_bias, axis=1, keepdims=True)] * rows, axis=0)
    out_row, in_row = iota((group_size * rows, head_rows), 0), iota((group_size * rows, head_rows), 1)
    gather = jnp.where(
        (out_row % rows == in_row // HEADS) & (out_row // rows == in_row % HEADS // KV_HEADS),
        1.0,
        0.0,
    ).astype(jnp.bfloat16)
    row_of = iota((head_rows, 1), 0) // HEADS
    lengths = jnp.zeros((head_rows, 1), jnp.int32)
    for b in range(rows):
        lengths = jnp.where(row_of == b, lengths_ref[:, b : b + 1], lengths)
    live = iota((head_rows, cache_len), 1) < lengths
    arrived(cache_sem.at[0], ck)
    for b in range(rows):
        kt[b] = ck[b].T
    arrived(cache_sem.at[1], cv)

    arrived(recv_sem.at[1], r2)
    total = r2[0].astype(jnp.float32)
    for p in range(1, chips):
        total = total + r2[p].astype(jnp.float32)
    queries = total
    spread = []
    for b in range(rows):
        wide = [
            jnp.broadcast_to(
                queries[b : b + 1, i * k_width : (i + 1) * k_width], (KV_HEADS, k_width)
            )
            for i in range(group_size)
        ]
        wide = jnp.where(own_group, jnp.concatenate(wide, axis=0), 0.0)
        mean = jnp.sum(wide * wide, axis=1, keepdims=True) / HEAD_DIM
        spread.append((wide * lax.rsqrt(mean + EPSILON) * query_gain).astype(jnp.bfloat16))
    scores = jnp.concatenate([dot(spread[b], kt[b]) for b in range(rows)], axis=0)
    scores = scores * HEAD_DIM ** (-0.5) + head_bias
    tail_log = jnp.log(1.0 + jnp.exp(-jnp.abs(scores)))
    remain = jnp.where(live, jnp.minimum(-scores, 0.0) - tail_log, 0.0)
    pieces = [remain[:, i * COLUMNS : (i + 1) * COLUMNS] for i in range(blocks)]
    highs = [block.astype(jnp.bfloat16) for block in pieces]
    lows = [
        (block - high.astype(jnp.float32)).astype(jnp.bfloat16)
        for block, high in zip(pieces, highs)
    ]
    sums = dot(jnp.concatenate(highs + lows, axis=0), later)
    after = [None] * blocks
    carry = jnp.zeros((head_rows, 1), jnp.float32)
    for i in reversed(range(blocks)):
        low = (blocks + i) * head_rows
        after[i] = (
            sums[i * head_rows : (i + 1) * head_rows] + sums[low : low + head_rows] + carry
        )
        carry = carry + jnp.sum(pieces[i], axis=1, keepdims=True)
    after_sum = jnp.concatenate(after, axis=1)
    chance = jnp.exp(jnp.minimum(scores, 0.0) - tail_log + after_sum)
    weight = jnp.where(live, chance, 0.0).astype(jnp.bfloat16)
    mixed_heads = jnp.concatenate(
        [dot(weight[b * HEADS : (b + 1) * HEADS], cv[b]) for b in range(rows)], axis=0
    )
    own_groups = jnp.concatenate([own_group] * rows, axis=0)
    heads = jnp.where(own_groups, mixed_heads, 0.0).astype(jnp.bfloat16)
    s3[...] = dot(gather, heads).astype(jnp.bfloat16)

    for k in furthest_first:
        send(2, peer_at[k], s3, r3.at[chip], recv_sem.at[2])

    arrived(recv_sem.at[3], r2kv)
    total = r2kv[0].astype(jnp.float32)
    for p in range(1, chips):
        total = total + r2kv[p].astype(jnp.float32)
    fresh_key = total[:, :k_width]
    new_value_ref[...] = total[:, k_width:].astype(jnp.bfloat16)
    squares = fresh_key * fresh_key
    key_lane = iota(squares.shape, 1) // HEAD_DIM
    key_scale = jnp.zeros_like(squares)
    for g in range(KV_HEADS):
        mean = jnp.sum(jnp.where(key_lane == g, squares, 0.0), axis=1, keepdims=True) / HEAD_DIM
        key_scale = jnp.where(key_lane == g, lax.rsqrt(mean + EPSILON), key_scale)
    new_key_ref[...] = (fresh_key * key_scale * key_gain).astype(jnp.bfloat16)
    for c in results[1:]:
        c.start()
    arrived(twin_sem.at[1], wo.at[core])
    arrived(twin_sem.at[2], gates_all.at[core])

    arrived(recv_sem.at[2], r3)
    for p in range(chips):
        block = r3[p].astype(jnp.float32)
        for i in range(group_size):
            attended_rows[p * rows : (p + 1) * rows, i * k_width : (i + 1) * k_width] = block[
                i * rows : (i + 1) * rows
            ]
    attended_all = attended_rows[...].astype(jnp.bfloat16)
    for h in range(2):
        columns = slice(h * share, (h + 1) * share)
        mixed = token_cols[:, columns] + dot(attended_all, wo[h])
        r4[chip, other, :, columns] = mixed.astype(jnp.bfloat16)

    mine = r4.at[chip, other]
    for k in range(chips):
        send(3, peer_at[k], mine, mine, direct_sem.at[k])
    pick = jnp.where(
        iota((8, half_rows), 1) == iota((8, half_rows), 0) + chip * rows, 1.0, 0.0
    ).astype(jnp.bfloat16)
    squares = jnp.zeros((all_rows, chip_share), jnp.float32)
    gate_column = gates_all[...].reshape(all_rows, 128)[:, :1]
    for which, b in enumerate((wg, wu)):
        arrived(weight_sem.at[which], b)
    arrived(weight_sem.at[2], wd)

    def chunks_of(group, squares, first, last):
        entries = []
        for k in group:
            source = chip_at[k]
            columns = pl.ds(pl.multiple_of(source * chip_share, chip_share), chip_share)
            if k:
                arrived(relay_sem.at[k - 1], r4.at[source, other])
            own_mixed[:, columns] = dot(pick, r4[source, core])[:rows]
            block = r4[source].reshape(all_rows, chip_share).astype(jnp.float32)
            squares = squares + block * block
            entries.append((columns, (block * ffn_gain_ref[:, columns]).astype(jnp.bfloat16)))
        if last:
            scale = lax.rsqrt(jnp.sum(squares, axis=1, keepdims=True) / width + EPSILON)
        for i in range(ff_share // COLUMNS):
            inner = slice(i * COLUMNS, (i + 1) * COLUMNS)
            gate_value = sum(dot(entry, wg[columns, inner]) for columns, entry in entries)
            up_value = sum(dot(entry, wu[columns, inner]) for columns, entry in entries)
            if not first:
                gate_value = gate_value + gate_acc[:, inner]
                up_value = up_value + up_acc[:, inner]
            if last:
                gate_value = gate_value * scale
                silu = gate_value / (1.0 + jnp.exp(-gate_value))
                hidden[:, inner] = (silu * (up_value * scale) * gate_column).astype(jnp.bfloat16)
            else:
                gate_acc[:, inner] = gate_value
                up_acc[:, inner] = up_value
        return squares

    for i, step in enumerate(SCHEDULE):
        if isinstance(step, int):
            block = r4.at[chip_at[step], core]
            arrived(direct_sem.at[step], block)
            if step:
                send(7, sibling, block, block, relay_sem.at[step - 1])
        else:
            squares = chunks_of(step, squares, step[0] == 0, i == len(SCHEDULE) - 1)

    step = width // DOWN_PARTS

    def spread_sums(part):
        arrived(pair_sem.at[part], p5.at[part])
        both = own5[part] + p5[part].astype(jnp.float32)
        for p in range(chips):
            t5[part, p] = both[p * rows : (p + 1) * rows].astype(jnp.bfloat16)
        for k in range(chips):
            send(9, peer_at[k], t5.at[part, chip_at[k]], r5.at[part, chip], spread_sem.at[part])

    for part in range(DOWN_PARTS):
        partial = dot(hidden[...], wd[:, part * step : (part + 1) * step])
        lower, upper = partial[:half_rows], partial[half_rows:]
        own5[part] = jnp.where(core == 0, upper, lower)
        s5[part] = jnp.where(core == 0, lower, upper).astype(jnp.bfloat16)
        send(8, sibling, s5.at[part], p5.at[part], pair_sem.at[part])
        if part > 1:
            spread_sums(part - 2)
    spread_sums(DOWN_PARTS - 2)
    spread_sums(DOWN_PARTS - 1)
    for part in range(DOWN_PARTS):
        arrived(spread_sem.at[part], r5.at[part])
        total = own_mixed[:, part * step : (part + 1) * step]
        for p in range(chips):
            total = total + r5[part, p].astype(jnp.float32)
        out_ref[:, part * step : (part + 1) * step] = total.astype(jnp.bfloat16)
    results[0].start()
    arrived(send_sem.at[0], s1)
    arrived(send_sem.at[1], s2)
    arrived(send_sem.at[10], s2kv)
    arrived(send_sem.at[2], r3)
    arrived(send_sem.at[3], r4.at[:, 0])
    arrived(send_sem.at[4], wqkv.at[my_rows])
    arrived(send_sem.at[5], wo.at[core])
    arrived(send_sem.at[6], gates_all.at[other])
    arrived(send_sem.at[7], r4.at[others, 0])
    arrived(send_sem.at[8], s5)
    arrived(send_sem.at[9], t5)
    for c in results:
        c.wait()


def local(
    n,
    tokens,
    lengths,
    cache_key,
    cache_value,
    routes,
    route_logits,
    mix_gain,
    query_gain,
    key_gain,
    head_bias,
    w_query,
    w_key,
    w_value,
    w_out,
    ffn_gain,
    w_gate,
    w_up,
    w_down,
):
    rows, width = tokens.shape
    chips = n // 2
    all_rows, half_rows = rows * n, rows * chips
    share, chip_share = width // n, width // chips
    q_width, k_width = w_query.shape[1], w_key.shape[1]
    wide = q_width + k_width + w_value.shape[1]
    step = width // DOWN_PARTS
    ff_share = w_gate.shape[1]
    anywhere = pl.BlockSpec(memory_space=pl.ANY)
    bf16, f32 = jnp.bfloat16, jnp.float32

    def like(array):
        return pltpu.VMEM(array.shape, array.dtype)

    flops = 2 * all_rows * 3 * w_gate.shape[0] * w_gate.shape[1]
    shapes = ((rows, width), (rows, k_width), (rows, w_value.shape[1]))
    results = pl.pallas_call(
        functools.partial(fused, n),
        out_shape=tuple(pltpu.VMEM(shape, bf16) for shape in shapes),
        in_specs=[anywhere] * 18,
        out_specs=(anywhere,) * 3,
        scratch_shapes=[
            like(tokens),
            pltpu.VMEM((1, rows), lengths.dtype),
            pltpu.VMEM(routes.shape[::-1], routes.dtype),
            pltpu.VMEM(route_logits.shape[::-1], f32),
            pltpu.VMEM((1, width), f32),
            pltpu.VMEM((1, HEAD_DIM), f32),
            pltpu.VMEM((1, HEAD_DIM), f32),
            pltpu.VMEM((1, HEADS), f32),
            pltpu.VMEM((1, width), f32),
            *(pltpu.VMEM(shape, bf16) for shape in shapes),
            like(w_query),
            pltpu.VMEM((chip_share, wide), bf16),
            pltpu.VMEM((2, *w_out.shape), bf16),
            like(cache_key),
            pltpu.VMEM((rows, k_width, cache_key.shape[1]), bf16),
            like(cache_value),
            like(w_gate),
            like(w_up),
            like(w_down),
            pltpu.VMEM((chips, 2 * rows, chip_share), bf16),
            pltpu.VMEM((chips, 2 * rows, chip_share), bf16),
            pltpu.VMEM((chips, rows, q_width), bf16),
            pltpu.VMEM((chips, rows, q_width), bf16),
            pltpu.VMEM((chips, rows, wide - q_width), bf16),
            pltpu.VMEM((chips, rows, wide - q_width), bf16),
            pltpu.VMEM((rows * q_width // k_width, k_width), bf16),
            pltpu.VMEM((chips, rows * q_width // k_width, k_width), bf16),
            pltpu.VMEM((chips, 2, half_rows, chip_share), bf16),
            pltpu.VMEM((DOWN_PARTS, half_rows, step), bf16),
            pltpu.VMEM((DOWN_PARTS, half_rows, step), bf16),
            pltpu.VMEM((DOWN_PARTS, half_rows, step), f32),
            pltpu.VMEM((DOWN_PARTS, chips, rows, step), bf16),
            pltpu.VMEM((DOWN_PARTS, chips, rows, step), bf16),
            pltpu.VMEM((2, half_rows, 128), f32),
            pltpu.VMEM((half_rows, chip_share), f32),
            pltpu.VMEM((half_rows, 128), f32),
            pltpu.VMEM((half_rows, q_width), f32),
            pltpu.VMEM((rows, width), f32),
            pltpu.VMEM((all_rows, ff_share), f32),
            pltpu.VMEM((all_rows, ff_share), f32),
            pltpu.VMEM((all_rows, ff_share), bf16),
            pltpu.SemaphoreType.DMA((9,)),
            pltpu.SemaphoreType.DMA((3,)),
            pltpu.SemaphoreType.DMA((4,)),
            pltpu.SemaphoreType.DMA((2,)),
            pltpu.SemaphoreType.DMA((3,)),
            pltpu.SemaphoreType.DMA((11,)),
            pltpu.SemaphoreType.DMA((4,)),
            pltpu.SemaphoreType.DMA((chips,)),
            pltpu.SemaphoreType.DMA((chips - 1,)),
            pltpu.SemaphoreType.DMA((DOWN_PARTS,)),
            pltpu.SemaphoreType.DMA((DOWN_PARTS,)),
            pltpu.SemaphoreType.DMA((3,)),
        ],
        compiler_params=pltpu.CompilerParams(
            collective_id=0, has_side_effects=True, vmem_limit_bytes=60 * 1024 * 1024
        ),
        cost_estimate=pl.CostEstimate(flops=flops, bytes_accessed=flops // all_rows, transcendentals=0),
    )(
        tokens,
        lengths.reshape(1, -1),
        cache_key,
        cache_value,
        routes.T,
        route_logits.T,
        mix_gain.reshape(1, -1),
        query_gain.reshape(1, -1),
        key_gain.reshape(1, -1),
        head_bias.reshape(1, -1),
        w_query,
        w_key,
        w_value,
        w_out,
        ffn_gain.reshape(1, -1),
        w_gate,
        w_up,
        w_down,
    )
    return pl.pallas_call(
        finish,
        out_shape=tuple(jax.ShapeDtypeStruct(shape, bf16) for shape in shapes),
        in_specs=[anywhere] * len(shapes),
        out_specs=(anywhere,) * len(shapes),
        scratch_shapes=[pltpu.SemaphoreType.DMA((len(shapes),))],
    )(*(pltpu.with_memory_space_constraint(result, pltpu.VMEM) for result in results))


def solution(mesh):
    n = mesh.shape["ep"]

    def body(*arrays):
        tokens, w_gate = arrays[0], arrays[15]
        share = tokens.shape[1] // n
        aligned = share == 128 and n & (n - 1) == 0 and n % 4 == 0
        halves = (FF // w_gate.shape[1]) % 2 == 0 and arrays[13].shape[1] == share
        if aligned and halves and w_gate.shape[1] % COLUMNS == 0 and tokens.shape[0] * n % 64 == 0:
            return local(n, *arrays)
        return plain(*arrays)

    return jax.shard_map(
        body,
        mesh=mesh,
        in_specs=(
            P(("grp", "ep"), None),
            P(("grp", "ep")),
            P(("grp", "ep"), None, None),
            P(("grp", "ep"), None, None),
            P(("grp", "ep"), None),
            P(("grp", "ep"), None),
            P(),
            P(),
            P(),
            P(),
            P("ep", None),
            P("ep", None),
            P("ep", None),
            P(None, "ep"),
            P(),
            P(None, "ep"),
            P(None, "ep"),
            P("ep", None),
        ),
        out_specs=(P(("grp", "ep"), None), P(("grp", "ep"), None), P(("grp", "ep"), None)),
        check_vma=False,
    )
```

```python
import functools

import jax
import jax.numpy as jnp
from jax import lax
from jax.experimental import pallas as pl
from jax.experimental.pallas import tpu as pltpu
from jax.sharding import PartitionSpec as P

HEADS = 16
KV_HEADS = 4
HEAD_DIM = 64
FF = 7168
EXPERTS = 4


EPSILON = 1e-06


def rms_scaled(values, gain):
    return values * lax.rsqrt(jnp.mean(values * values, axis=-1, keepdims=True) + EPSILON) * gain


def route_weights(routes, route_logits):
    experts_iota = jnp.arange(EXPERTS, dtype=jnp.int32)[None, :]
    first_share = jax.nn.sigmoid(route_logits[:, 0:1] - route_logits[:, 1:2])
    second_share = jax.nn.sigmoid(route_logits[:, 1:2] - route_logits[:, 0:1])
    return jnp.where(routes[:, 0:1] == experts_iota, first_share, 0.0) + jnp.where(
        routes[:, 1:2] == experts_iota, second_share, 0.0
    )


def stick_attend(queries, lengths, cache_key, cache_value, query_gain, head_bias):
    batch_rows = queries.shape[0]
    cache_len = cache_key.shape[1]
    group_size = HEADS // KV_HEADS
    normed_query = rms_scaled(queries.reshape(batch_rows, HEADS, HEAD_DIM), query_gain).astype(
        jnp.bfloat16
    )
    normed_query = normed_query.reshape(batch_rows, KV_HEADS, group_size, HEAD_DIM)
    key_heads = cache_key.reshape(batch_rows, cache_len, KV_HEADS, HEAD_DIM)
    value_heads = cache_value.reshape(batch_rows, cache_len, KV_HEADS, HEAD_DIM)
    scores = jnp.einsum(
        "bkgd,blkd->bkgl", normed_query, key_heads, preferred_element_type=jnp.float32
    ) * HEAD_DIM ** (-0.5)
    scores = scores + head_bias.reshape(KV_HEADS, group_size)[None, :, :, None]
    live_mask = (
        jnp.arange(cache_len, dtype=jnp.int32)[None, None, None, :] < lengths[:, None, None, None]
    )
    remain = jnp.where(live_mask, jax.nn.log_sigmoid(-scores), 0.0)
    after_sum = lax.cumsum(remain, axis=3, reverse=True) - remain
    weights = jnp.where(live_mask, jnp.exp(jax.nn.log_sigmoid(scores) + after_sum), 0.0).astype(
        jnp.bfloat16
    )
    attended = jnp.einsum(
        "bkgl,blkd->bkgd", weights, value_heads, preferred_element_type=jnp.float32
    )
    return attended.reshape(batch_rows, HEADS * HEAD_DIM).astype(jnp.bfloat16)


def plain(
    tokens,
    lengths,
    cache_key,
    cache_value,
    routes,
    route_logits,
    mix_gain,
    query_gain,
    key_gain,
    head_bias,
    w_query,
    w_key,
    w_value,
    w_out,
    ffn_gain,
    w_gate,
    w_up,
    w_down,
):
    token_rows = tokens.shape[0]
    key_width = w_key.shape[1]
    as_float = tokens.astype(jnp.float32)
    normed = rms_scaled(as_float, mix_gain).astype(jnp.bfloat16)
    pieces = (
        lax.all_gather(w_query, "ep", axis=0, tiled=True),
        lax.all_gather(w_key, "ep", axis=0, tiled=True),
        lax.all_gather(w_value, "ep", axis=0, tiled=True),
    )
    queries, fresh_key, fresh_value = tuple(
        (jnp.dot(normed, weight, preferred_element_type=jnp.float32) for weight in pieces)
    )
    new_key = rms_scaled(fresh_key.reshape(token_rows, KV_HEADS, HEAD_DIM), key_gain)
    new_key = new_key.reshape(token_rows, key_width).astype(jnp.bfloat16)
    new_value = fresh_value.astype(jnp.bfloat16)
    attended = stick_attend(queries, lengths, cache_key, cache_value, query_gain, head_bias)
    mixed = as_float + jnp.dot(
        attended,
        lax.all_gather(w_out, "ep", axis=1, tiled=True),
        preferred_element_type=jnp.float32,
    )
    expert_in = rms_scaled(mixed, ffn_gain).astype(jnp.bfloat16)
    every_gate = lax.all_gather(route_weights(routes, route_logits), "ep", axis=0, tiled=True)
    ff_share = w_gate.shape[1]
    my_expert = lax.axis_index("ep") // (FF // ff_share)
    my_gate = lax.dynamic_slice_in_dim(every_gate, my_expert, 1, 1)
    input_rows = lax.all_gather(expert_in, "ep", axis=0, tiled=True)
    gate_value = jnp.dot(input_rows, w_gate, preferred_element_type=jnp.float32)
    up_value = jnp.dot(input_rows, w_up, preferred_element_type=jnp.float32)
    hidden = (jax.nn.silu(gate_value) * up_value * my_gate).astype(jnp.bfloat16)
    expert_sum = lax.psum_scatter(
        jnp.dot(hidden, w_down, preferred_element_type=jnp.float32),
        "ep",
        scatter_dimension=0,
        tiled=True,
    )
    return ((mixed + expert_sum).astype(jnp.bfloat16), new_key, new_value)


WEIGHT_PARTS = 2
PAIR_LAG = 2
DOWN_WIDTHS = (512, 512, 512, 512)
SCHEDULE = (0, (0,), 1, 2, 3, 4, (1,), 5, (2,), 6, (3,), 7, (4,), (5, 6), (7,))
COLUMNS = 256


def dot(left, right):
    return jnp.dot(left, right, preferred_element_type=jnp.float32)


def iota(shape, dim):
    return lax.broadcasted_iota(jnp.int32, shape, dim)


def column(row):
    square = (row.shape[1], row.shape[1])
    return jnp.sum(
        jnp.where(iota(square, 0) == iota(square, 1), jnp.broadcast_to(row, square), 0.0),
        axis=1,
        keepdims=True,
    )


def finish(*refs):
    half = len(refs) // 2
    copies = [
        pltpu.make_async_copy(refs[i], refs[half + i], refs[-1].at[i]) for i in range(half)
    ]
    for copy in copies:
        copy.start()
    for copy in copies:
        copy.wait()


def fused(
    n,
    tokens_hbm,
    lengths_hbm,
    ck_hbm,
    cv_hbm,
    routes_hbm,
    logits_hbm,
    mix_gain_hbm,
    query_gain_hbm,
    key_gain_hbm,
    head_bias_hbm,
    wq_hbm,
    wk_hbm,
    wv_hbm,
    wo_hbm,
    ffn_gain_hbm,
    wg_hbm,
    wu_hbm,
    wd_hbm,
    out_any,
    new_key_any,
    new_value_any,
    tokens_ref,
    lengths_ref,
    routes_ref,
    logits_ref,
    mix_gain_ref,
    query_gain_ref,
    key_gain_ref,
    head_bias_ref,
    ffn_gain_ref,
    out_ref,
    new_key_ref,
    new_value_ref,
    wq_raw,
    wqkv,
    wo,
    ck,
    kt,
    cv,
    wg,
    wu,
    wd,
    s1,
    r1,
    s2,
    r2,
    s2kv,
    r2kv,
    s3,
    r3,
    r4,
    s5,
    p5,
    own5,
    t5,
    r5,
    gates_all,
    token_cols,
    aux_rows,
    attended_rows,
    own_mixed,
    gate_acc,
    up_acc,
    hidden,
    operand_sem,
    small_sem,
    send_sem,
    recv_sem,
    direct_sem,
    relay_sem,
    pair_sem,
    spread_sem,
    twin_sem,
):
    me = lax.axis_index("ep")
    core, chip = me % 2, me // 2
    chips = n // 2
    other = 1 - core
    sibling = 2 * chip + other
    rows, width = tokens_ref.shape
    half_rows = rows * chips
    all_rows = rows * n
    share = width // n
    chip_share = width // chips
    q_width, k_width = wq_hbm.shape[1], wk_hbm.shape[1]
    cache_len = ck.shape[1]
    group_size = HEADS // KV_HEADS
    ff_share = wg.shape[1]
    my_expert = me // (FF // ff_share)

    barrier = pltpu.get_barrier_semaphore()
    chip_at = [chip]
    for k in range(1, chips):
        bit = k.bit_length() - 1
        flip = 2**bit * (1 - 2 * ((chip // 2**bit) % 2))
        chip_at.append(chip_at[k - 2**bit] + flip)
    peer_at = [2 * c + other for c in chip_at]
    furthest_first = range(chips - 1, -1, -1)
    for k in furthest_first:
        pl.semaphore_signal(
            barrier,
            inc=1,
            device_id={"ep": peer_at[k]},
            device_id_type=pl.DeviceIdType.MESH,
        )

    operands = [
        pltpu.make_async_copy(a, b, operand_sem.at[i])
        for i, (a, b) in enumerate(
            (
                (tokens_hbm, tokens_ref),
                (routes_hbm, routes_ref),
                (logits_hbm, logits_ref),
                (mix_gain_hbm, mix_gain_ref),
                (query_gain_hbm, query_gain_ref),
                (key_gain_hbm, key_gain_ref),
                (head_bias_hbm, head_bias_ref),
                (ffn_gain_hbm, ffn_gain_ref),
                (lengths_hbm, lengths_ref),
            )
        )
    ]
    for c in operands:
        c.start()

    my_rows = pl.ds(pl.multiple_of(core * share, share), share)
    small = [
        pltpu.make_async_copy(a, b, small_sem.at[i])
        for i, (a, b) in enumerate(
            (
                (wq_hbm, wq_raw),
                (wk_hbm, wqkv.at[my_rows, q_width : q_width + k_width]),
                (wv_hbm, wqkv.at[my_rows, q_width + k_width :]),
            )
        )
    ]
    for head in range(HEADS):
        place = head % group_size * KV_HEADS + head // group_size
        small.append(
            pltpu.make_async_copy(
                wo_hbm.at[head * HEAD_DIM : (head + 1) * HEAD_DIM],
                wo.at[core, place * HEAD_DIM : (place + 1) * HEAD_DIM],
                small_sem.at[3],
            )
        )
    for c in small:
        c.start()
    caches = [pltpu.make_async_copy(ck_hbm.at[b], ck.at[b], operand_sem.at[0]) for b in range(rows)]
    caches += [pltpu.make_async_copy(cv_hbm.at[b], cv.at[b], operand_sem.at[1]) for b in range(rows)]
    weights = []
    for which, (a, b) in enumerate(((wg_hbm, wg), (wu_hbm, wu), (wd_hbm, wd))):
        step = b.shape[0] // WEIGHT_PARTS
        for part in range(WEIGHT_PARTS):
            piece = pl.ds(part * step, step)
            weights.append(pltpu.make_async_copy(a.at[piece], b.at[piece], operand_sem.at[2 + which]))

    results = [
        pltpu.make_async_copy(a, b, operand_sem.at[5 + i])
        for i, (a, b) in enumerate(
            ((out_ref, out_any), (new_key_ref, new_key_any), (new_value_ref, new_value_any))
        )
    ]
    for c in operands:
        c.wait()

    def send(stage, device, source, target, arrival):
        pltpu.make_async_remote_copy(
            src_ref=source,
            dst_ref=target,
            send_sem=send_sem.at[stage],
            recv_sem=arrival,
            device_id={"ep": device},
            device_id_type=pl.DeviceIdType.MESH,
        ).start()

    def arrived(sem, blocks):
        pltpu.make_async_copy(blocks, blocks, sem).wait()

    others = pl.ds(0, chips - 1)

    as_float = tokens_ref[...].astype(jnp.float32)
    scale = lax.rsqrt(jnp.mean(as_float * as_float, axis=1, keepdims=True) + EPSILON)
    lane = iota((rows, 128), 1)
    logit_gap = column(logits_ref[0:1] - logits_ref[1:2])
    chosen = [column(routes_ref[i : i + 1].astype(jnp.float32)) for i in range(2)]
    first_share = 1.0 / (1.0 + jnp.exp(-logit_gap))
    second_share = 1.0 / (1.0 + jnp.exp(logit_gap))
    expert_lane = (lane % EXPERTS).astype(jnp.float32)
    gates = jnp.where(chosen[0] == expert_lane, first_share, 0.0) + jnp.where(
        chosen[1] == expert_lane, second_share, 0.0
    )
    aux = jnp.where(lane < 3 * EXPERTS, gates, scale)
    high = aux.astype(jnp.bfloat16).astype(jnp.float32)
    middle = (aux - high).astype(jnp.bfloat16).astype(jnp.float32)
    low = aux - high - middle
    term = jnp.where(lane < 3 * EXPERTS, lane // EXPERTS, lane - 3 * EXPERTS)
    aux = jnp.where(term == 0, high, jnp.where(term == 1, middle, low))
    aux = jnp.concatenate([aux] * (chip_share // 128), axis=1)
    for p in range(chips):
        s1[p] = jnp.concatenate(
            [as_float[:, p * chip_share : (p + 1) * chip_share], aux], axis=0
        ).astype(jnp.bfloat16)
    for c in small[:3]:
        c.wait()
    left_half = iota((share, 2 * HEAD_DIM), 1) < HEAD_DIM
    for place in range(0, HEADS, 2):
        halves = []
        for side in range(2):
            head = (place + side) % KV_HEADS * group_size + (place + side) // KV_HEADS
            start = head // 2 * 2 * HEAD_DIM
            half = wq_raw[:, start : start + 2 * HEAD_DIM].astype(jnp.float32)
            halves.append(half if head % 2 == side else pltpu.roll(half, HEAD_DIM, 1))
        wqkv[my_rows, place * HEAD_DIM : (place + 2) * HEAD_DIM] = jnp.where(
            left_half, halves[0], halves[1]
        ).astype(jnp.bfloat16)
    pl.semaphore_wait(barrier, chips)
    for k in furthest_first:
        send(0, peer_at[k], s1.at[chip_at[k]], r1.at[chip], recv_sem.at[0])
    query_half = wqkv.at[my_rows, 0:q_width]
    send(4, sibling, query_half, query_half, twin_sem.at[0])
    for c in caches:
        c.start()
    arrived(recv_sem.at[0], r1)
    for c in weights:
        c.start()
    for p in range(chips):
        block = r1[p].astype(jnp.float32)
        token_cols[p * rows : (p + 1) * rows, :] = block[:rows]
        aux_rows[p * rows : (p + 1) * rows, :] = block[rows:, :128]
    aux = aux_rows[...]
    lane = iota(aux.shape, 1)
    row_scale = jnp.sum(
        jnp.where((lane >= 3 * EXPERTS) & (lane < 3 * EXPERTS + 3), aux, 0.0), axis=1, keepdims=True
    )
    my_gain = mix_gain_ref[:, pl.ds(pl.multiple_of(chip * chip_share, chip_share), chip_share)]
    normed = (token_cols[...] * row_scale * my_gain).astype(jnp.bfloat16)
    arrived(twin_sem.at[0], query_half)

    partial = dot(normed, wqkv[:, :q_width])
    for p in range(chips):
        s2[p] = partial[p * rows : (p + 1) * rows].astype(jnp.bfloat16)
    for k in furthest_first:
        send(1, peer_at[k], s2.at[chip_at[k]], r2.at[chip], recv_sem.at[1])
    key_value_half = wqkv.at[my_rows, q_width:]
    send(3, sibling, key_value_half, key_value_half, twin_sem.at[3])
    my_gate = jnp.sum(
        jnp.where((lane < 3 * EXPERTS) & (lane % EXPERTS == my_expert), aux, 0.0),
        axis=1,
        keepdims=True,
    )
    gates_all[other] = jnp.broadcast_to(my_gate, aux.shape)
    send(5, sibling, gates_all.at[other], gates_all.at[other], twin_sem.at[2])

    own_group = iota((HEADS, k_width), 1) // HEAD_DIM == iota((HEADS, k_width), 0) % KV_HEADS
    later = jnp.where(
        iota((COLUMNS, COLUMNS), 0) > iota((COLUMNS, COLUMNS), 1), 1.0, 0.0
    ).astype(jnp.bfloat16)
    query_gain = jnp.concatenate([query_gain_ref[...]] * KV_HEADS, axis=1)
    key_gain = jnp.concatenate([key_gain_ref[...]] * KV_HEADS, axis=1)
    blocks = cache_len // COLUMNS
    head_rows = rows * HEADS
    place, head = iota((HEADS, HEADS), 0), iota((HEADS, HEADS), 1)
    head_bias = jnp.where(
        head == place % KV_HEADS * group_size + place // KV_HEADS,
        jnp.broadcast_to(head_bias_ref[...], head.shape),
        0.0,
    )
    head_bias = jnp.concatenate([jnp.sum(head_bias, axis=1, keepdims=True)] * rows, axis=0)
    out_row, in_row = iota((group_size * rows, head_rows), 0), iota((group_size * rows, head_rows), 1)
    gather = jnp.where(
        (out_row % rows == in_row // HEADS) & (out_row // rows == in_row % HEADS // KV_HEADS),
        1.0,
        0.0,
    ).astype(jnp.bfloat16)
    row_of = iota((head_rows, 1), 0) // HEADS
    lengths = jnp.zeros((head_rows, 1), jnp.int32)
    for b in range(rows):
        lengths = jnp.where(row_of == b, lengths_ref[:, b : b + 1], lengths)
    live = iota((head_rows, cache_len), 1) < lengths
    arrived(operand_sem.at[0], ck)
    for b in range(rows):
        kt[b] = ck[b].T
    arrived(operand_sem.at[1], cv)

    arrived(twin_sem.at[3], key_value_half)
    partial = dot(normed, wqkv[:, q_width:])
    for p in range(chips):
        s2kv[p] = partial[p * rows : (p + 1) * rows].astype(jnp.bfloat16)
    arrived(recv_sem.at[1], r2)
    for k in furthest_first:
        send(2, peer_at[k], s2kv.at[chip_at[k]], r2kv.at[chip], recv_sem.at[3])
    arrived(small_sem.at[3], wo.at[core])
    arrived(send_sem.at[4], query_half)
    send(4, sibling, wo.at[core], wo.at[core], twin_sem.at[1])
    total = r2[0].astype(jnp.float32)
    for p in range(1, chips):
        total = total + r2[p].astype(jnp.float32)
    queries = total
    spread = []
    for b in range(rows):
        wide = [
            jnp.broadcast_to(
                queries[b : b + 1, i * k_width : (i + 1) * k_width], (KV_HEADS, k_width)
            )
            for i in range(group_size)
        ]
        wide = jnp.where(own_group, jnp.concatenate(wide, axis=0), 0.0)
        mean = jnp.sum(wide * wide, axis=1, keepdims=True) / HEAD_DIM
        spread.append((wide * lax.rsqrt(mean + EPSILON) * query_gain).astype(jnp.bfloat16))
    scores = jnp.concatenate([dot(spread[b], kt[b]) for b in range(rows)], axis=0)
    scores = scores * HEAD_DIM ** (-0.5) + head_bias
    tail_log = jnp.log(1.0 + jnp.exp(-jnp.abs(scores)))
    remain = jnp.where(live, jnp.minimum(-scores, 0.0) - tail_log, 0.0)
    pieces = [remain[:, i * COLUMNS : (i + 1) * COLUMNS] for i in range(blocks)]
    highs = [block.astype(jnp.bfloat16) for block in pieces]
    lows = [
        (block - high.astype(jnp.float32)).astype(jnp.bfloat16)
        for block, high in zip(pieces, highs)
    ]
    sums = dot(jnp.concatenate(highs + lows, axis=0), later)
    after = [None] * blocks
    carry = jnp.zeros((head_rows, 1), jnp.float32)
    for i in reversed(range(blocks)):
        low = (blocks + i) * head_rows
        after[i] = (
            sums[i * head_rows : (i + 1) * head_rows] + sums[low : low + head_rows] + carry
        )
        carry = carry + jnp.sum(pieces[i], axis=1, keepdims=True)
    after_sum = jnp.concatenate(after, axis=1)
    chance = jnp.exp(jnp.minimum(scores, 0.0) - tail_log + after_sum)
    weight = jnp.where(live, chance, 0.0).astype(jnp.bfloat16)
    mixed_heads = jnp.concatenate(
        [dot(weight[b * HEADS : (b + 1) * HEADS], cv[b]) for b in range(rows)], axis=0
    )
    own_groups = jnp.concatenate([own_group] * rows, axis=0)
    heads = jnp.where(own_groups, mixed_heads, 0.0).astype(jnp.bfloat16)
    s3[...] = dot(gather, heads).astype(jnp.bfloat16)

    arrived(send_sem.at[0], s1)
    for k in furthest_first:
        send(0, peer_at[k], s3, r3.at[chip], recv_sem.at[2])

    arrived(twin_sem.at[1], wo.at[core])
    arrived(twin_sem.at[2], gates_all.at[core])

    arrived(recv_sem.at[2], r3)
    for p in range(chips):
        block = r3[p].astype(jnp.float32)
        for i in range(group_size):
            attended_rows[p * rows : (p + 1) * rows, i * k_width : (i + 1) * k_width] = block[
                i * rows : (i + 1) * rows
            ]
    attended_all = attended_rows[...].astype(jnp.bfloat16)
    for h in range(2):
        columns = slice(h * share, (h + 1) * share)
        mixed = token_cols[:, columns] + dot(attended_all, wo[h])
        r4[chip, other, :, columns] = mixed.astype(jnp.bfloat16)

    mine = r4.at[chip, other]
    arrived(send_sem.at[1], s2)
    arrived(send_sem.at[5], gates_all.at[other])
    for k in range(chips):
        send(1, peer_at[k], mine, mine, direct_sem.at[k])
    pick = jnp.where(
        iota((8, half_rows), 1) == iota((8, half_rows), 0) + chip * rows, 1.0, 0.0
    ).astype(jnp.bfloat16)
    squares = jnp.zeros((all_rows, chip_share), jnp.float32)
    gate_column = gates_all[...].reshape(all_rows, 128)[:, :1]
    for which, b in enumerate((wg, wu)):
        arrived(operand_sem.at[2 + which], b)
    arrived(operand_sem.at[4], wd)

    def chunks_of(group, squares, first, last):
        entries = []
        for k in group:
            source = chip_at[k]
            columns = pl.ds(pl.multiple_of(source * chip_share, chip_share), chip_share)
            if k:
                arrived(relay_sem.at[k - 1], r4.at[source, other])
            own_mixed[:, columns] = dot(pick, r4[source, core])[:rows]
            block = r4[source].reshape(all_rows, chip_share).astype(jnp.float32)
            squares = squares + block * block
            entries.append((columns, (block * ffn_gain_ref[:, columns]).astype(jnp.bfloat16)))
        if last:
            scale = lax.rsqrt(jnp.sum(squares, axis=1, keepdims=True) / width + EPSILON)
        for i in range(ff_share // COLUMNS):
            inner = slice(i * COLUMNS, (i + 1) * COLUMNS)
            gate_value = sum(dot(entry, wg[columns, inner]) for columns, entry in entries)
            up_value = sum(dot(entry, wu[columns, inner]) for columns, entry in entries)
            if not first:
                gate_value = gate_value + gate_acc[:, inner]
                up_value = up_value + up_acc[:, inner]
            if last:
                gate_value = gate_value * scale
                silu = gate_value / (1.0 + jnp.exp(-gate_value))
                hidden[:, inner] = (silu * (up_value * scale) * gate_column).astype(jnp.bfloat16)
            else:
                gate_acc[:, inner] = gate_value
                up_acc[:, inner] = up_value
        return squares

    def finish_key_value():
        arrived(recv_sem.at[3], r2kv)
        total = r2kv[0].astype(jnp.float32)
        for p in range(1, chips):
            total = total + r2kv[p].astype(jnp.float32)
        fresh_key = total[:, :k_width]
        new_value_ref[...] = total[:, k_width:].astype(jnp.bfloat16)
        key_squares = fresh_key * fresh_key
        key_lane = iota(key_squares.shape, 1) // HEAD_DIM
        key_scale = jnp.zeros_like(key_squares)
        for g in range(KV_HEADS):
            mean = jnp.sum(jnp.where(key_lane == g, key_squares, 0.0), axis=1, keepdims=True) / HEAD_DIM
            key_scale = jnp.where(key_lane == g, lax.rsqrt(mean + EPSILON), key_scale)
        new_key_ref[...] = (fresh_key * key_scale * key_gain).astype(jnp.bfloat16)
        for c in results[1:]:
            c.start()

    for i, step in enumerate(SCHEDULE):
        if i == 2:
            finish_key_value()
        if isinstance(step, int):
            block = r4.at[chip_at[step], core]
            arrived(direct_sem.at[step], block)
            if step:
                send(6, sibling, block, block, relay_sem.at[step - 1])
        else:
            squares = chunks_of(step, squares, step[0] == 0, i == len(SCHEDULE) - 1)

    parts = len(DOWN_WIDTHS)
    starts = [sum(DOWN_WIDTHS[:part]) for part in range(parts)]

    def spread_sums(part):
        lanes = pl.ds(0, DOWN_WIDTHS[part])
        arrived(pair_sem.at[part], p5.at[part, :, lanes])
        both = own5[part, :, lanes] + p5[part, :, lanes].astype(jnp.float32)
        for p in range(chips):
            t5[part, p, :, lanes] = both[p * rows : (p + 1) * rows].astype(jnp.bfloat16)
        for k in range(chips):
            send(
                7,
                peer_at[k],
                t5.at[part, chip_at[k], :, lanes],
                r5.at[part, chip, :, lanes],
                spread_sem.at[part],
            )

    def down_product(start, lanes):
        return jnp.concatenate(
            [
                dot(hidden[...], wd[:, start + i : start + i + COLUMNS])
                for i in range(0, lanes, COLUMNS)
            ],
            axis=1,
        )

    for part in range(parts):
        lanes = pl.ds(0, DOWN_WIDTHS[part])
        partial = down_product(starts[part], DOWN_WIDTHS[part])
        lower, upper = partial[:half_rows], partial[half_rows:]
        own5[part, :, lanes] = jnp.where(core == 0, upper, lower)
        s5[part, :, lanes] = jnp.where(core == 0, lower, upper).astype(jnp.bfloat16)
        send(5, sibling, s5.at[part, :, lanes], p5.at[part, :, lanes], pair_sem.at[part])
        if part >= PAIR_LAG:
            spread_sums(part - PAIR_LAG)
    for part in range(parts - PAIR_LAG, parts):
        spread_sums(part)
    for part in range(parts):
        lanes = pl.ds(0, DOWN_WIDTHS[part])
        columns = slice(starts[part], starts[part] + DOWN_WIDTHS[part])
        arrived(spread_sem.at[part], r5.at[part, :, :, lanes])
        total = own_mixed[:, columns]
        for p in range(chips):
            total = total + r5[part, p, :, lanes].astype(jnp.float32)
        out_ref[:, columns] = total.astype(jnp.bfloat16)
    results[0].start()
    arrived(send_sem.at[2], s2kv)
    arrived(send_sem.at[3], key_value_half)
    arrived(send_sem.at[0], r3)
    arrived(send_sem.at[1], r4.at[:, 0])
    arrived(send_sem.at[4], wo.at[core])
    arrived(send_sem.at[6], r4.at[others, 0])
    whole = pl.ds(0, width // s5.shape[2])
    arrived(send_sem.at[5], s5.at[whole])
    arrived(send_sem.at[7], t5.at[whole])
    for c in results:
        c.wait()


def local(
    n,
    tokens,
    lengths,
    cache_key,
    cache_value,
    routes,
    route_logits,
    mix_gain,
    query_gain,
    key_gain,
    head_bias,
    w_query,
    w_key,
    w_value,
    w_out,
    ffn_gain,
    w_gate,
    w_up,
    w_down,
):
    rows, width = tokens.shape
    chips = n // 2
    all_rows, half_rows = rows * n, rows * chips
    share, chip_share = width // n, width // chips
    q_width, k_width = w_query.shape[1], w_key.shape[1]
    wide = q_width + k_width + w_value.shape[1]
    parts, step = len(DOWN_WIDTHS), max(DOWN_WIDTHS)
    ff_share = w_gate.shape[1]
    anywhere = pl.BlockSpec(memory_space=pl.ANY)
    bf16, f32 = jnp.bfloat16, jnp.float32

    def like(array):
        return pltpu.VMEM(array.shape, array.dtype)

    flops = 2 * all_rows * 3 * w_gate.shape[0] * w_gate.shape[1]
    shapes = ((rows, width), (rows, k_width), (rows, w_value.shape[1]))
    results = pl.pallas_call(
        functools.partial(fused, n),
        out_shape=tuple(pltpu.VMEM(shape, bf16) for shape in shapes),
        in_specs=[anywhere] * 18,
        out_specs=(anywhere,) * 3,
        scratch_shapes=[
            like(tokens),
            pltpu.VMEM((1, rows), lengths.dtype),
            pltpu.VMEM(routes.shape[::-1], routes.dtype),
            pltpu.VMEM(route_logits.shape[::-1], f32),
            pltpu.VMEM((1, width), f32),
            pltpu.VMEM((1, HEAD_DIM), f32),
            pltpu.VMEM((1, HEAD_DIM), f32),
            pltpu.VMEM((1, HEADS), f32),
            pltpu.VMEM((1, width), f32),
            *(pltpu.VMEM(shape, bf16) for shape in shapes),
            like(w_query),
            pltpu.VMEM((chip_share, wide), bf16),
            pltpu.VMEM((2, *w_out.shape), bf16),
            like(cache_key),
            pltpu.VMEM((rows, k_width, cache_key.shape[1]), bf16),
            like(cache_value),
            like(w_gate),
            like(w_up),
            like(w_down),
            pltpu.VMEM((chips, 2 * rows, chip_share), bf16),
            pltpu.VMEM((chips, 2 * rows, chip_share), bf16),
            pltpu.VMEM((chips, rows, q_width), bf16),
            pltpu.VMEM((chips, rows, q_width), bf16),
            pltpu.VMEM((chips, rows, wide - q_width), bf16),
            pltpu.VMEM((chips, rows, wide - q_width), bf16),
            pltpu.VMEM((rows * q_width // k_width, k_width), bf16),
            pltpu.VMEM((chips, rows * q_width // k_width, k_width), bf16),
            pltpu.VMEM((chips, 2, half_rows, chip_share), bf16),
            pltpu.VMEM((parts, half_rows, step), bf16),
            pltpu.VMEM((parts, half_rows, step), bf16),
            pltpu.VMEM((parts, half_rows, step), f32),
            pltpu.VMEM((parts, chips, rows, step), bf16),
            pltpu.VMEM((parts, chips, rows, step), bf16),
            pltpu.VMEM((2, half_rows, 128), f32),
            pltpu.VMEM((half_rows, chip_share), f32),
            pltpu.VMEM((half_rows, 128), f32),
            pltpu.VMEM((half_rows, q_width), f32),
            pltpu.VMEM((rows, width), f32),
            pltpu.VMEM((all_rows, ff_share), f32),
            pltpu.VMEM((all_rows, ff_share), f32),
            pltpu.VMEM((all_rows, ff_share), bf16),
            pltpu.SemaphoreType.DMA((9,)),
            pltpu.SemaphoreType.DMA((4,)),
            pltpu.SemaphoreType.DMA((8,)),
            pltpu.SemaphoreType.DMA((4,)),
            pltpu.SemaphoreType.DMA((chips,)),
            pltpu.SemaphoreType.DMA((chips - 1,)),
            pltpu.SemaphoreType.DMA((parts,)),
            pltpu.SemaphoreType.DMA((parts,)),
            pltpu.SemaphoreType.DMA((4,)),
        ],
        compiler_params=pltpu.CompilerParams(
            collective_id=0, has_side_effects=True, vmem_limit_bytes=60 * 1024 * 1024
        ),
        cost_estimate=pl.CostEstimate(flops=flops, bytes_accessed=flops // all_rows, transcendentals=0),
    )(
        tokens,
        lengths.reshape(1, -1),
        cache_key,
        cache_value,
        routes.T,
        route_logits.T,
        mix_gain.reshape(1, -1),
        query_gain.reshape(1, -1),
        key_gain.reshape(1, -1),
        head_bias.reshape(1, -1),
        w_query,
        w_key,
        w_value,
        w_out,
        ffn_gain.reshape(1, -1),
        w_gate,
        w_up,
        w_down,
    )
    return pl.pallas_call(
        finish,
        out_shape=tuple(jax.ShapeDtypeStruct(shape, bf16) for shape in shapes),
        in_specs=[anywhere] * len(shapes),
        out_specs=(anywhere,) * len(shapes),
        scratch_shapes=[pltpu.SemaphoreType.DMA((len(shapes),))],
    )(*(pltpu.with_memory_space_constraint(result, pltpu.VMEM) for result in results))


def solution(mesh):
    n = mesh.shape["ep"]

    def body(*arrays):
        tokens, w_gate = arrays[0], arrays[15]
        share = tokens.shape[1] // n
        aligned = share == 128 and n & (n - 1) == 0 and n % 4 == 0
        halves = (FF // w_gate.shape[1]) % 2 == 0 and arrays[13].shape[1] == share
        if aligned and halves and w_gate.shape[1] % COLUMNS == 0 and tokens.shape[0] * n % 64 == 0 and tokens.shape[1] == sum(DOWN_WIDTHS):
            return local(n, *arrays)
        return plain(*arrays)

    return jax.shard_map(
        body,
        mesh=mesh,
        in_specs=(
            P(("grp", "ep"), None),
            P(("grp", "ep")),
            P(("grp", "ep"), None, None),
            P(("grp", "ep"), None, None),
            P(("grp", "ep"), None),
            P(("grp", "ep"), None),
            P(),
            P(),
            P(),
            P(),
            P("ep", None),
            P("ep", None),
            P("ep", None),
            P(None, "ep"),
            P(),
            P(None, "ep"),
            P(None, "ep"),
            P("ep", None),
        ),
        out_specs=(P(("grp", "ep"), None), P(("grp", "ep"), None), P(("grp", "ep"), None)),
        check_vma=False,
    )
```

```python
import functools

import jax
import jax.numpy as jnp
from jax import lax
from jax.experimental import pallas as pl
from jax.experimental.pallas import tpu as pltpu
from jax.sharding import PartitionSpec as P

HEADS = 16
KV_HEADS = 4
HEAD_DIM = 64
FF = 7168
EXPERTS = 4


EPSILON = 1e-06


def rms_scaled(values, gain):
    return values * lax.rsqrt(jnp.mean(values * values, axis=-1, keepdims=True) + EPSILON) * gain


def route_weights(routes, route_logits):
    experts_iota = jnp.arange(EXPERTS, dtype=jnp.int32)[None, :]
    first_share = jax.nn.sigmoid(route_logits[:, 0:1] - route_logits[:, 1:2])
    second_share = jax.nn.sigmoid(route_logits[:, 1:2] - route_logits[:, 0:1])
    return jnp.where(routes[:, 0:1] == experts_iota, first_share, 0.0) + jnp.where(
        routes[:, 1:2] == experts_iota, second_share, 0.0
    )


def stick_attend(queries, lengths, cache_key, cache_value, query_gain, head_bias):
    batch_rows = queries.shape[0]
    cache_len = cache_key.shape[1]
    group_size = HEADS // KV_HEADS
    normed_query = rms_scaled(queries.reshape(batch_rows, HEADS, HEAD_DIM), query_gain).astype(
        jnp.bfloat16
    )
    normed_query = normed_query.reshape(batch_rows, KV_HEADS, group_size, HEAD_DIM)
    key_heads = cache_key.reshape(batch_rows, cache_len, KV_HEADS, HEAD_DIM)
    value_heads = cache_value.reshape(batch_rows, cache_len, KV_HEADS, HEAD_DIM)
    scores = jnp.einsum(
        "bkgd,blkd->bkgl", normed_query, key_heads, preferred_element_type=jnp.float32
    ) * HEAD_DIM ** (-0.5)
    scores = scores + head_bias.reshape(KV_HEADS, group_size)[None, :, :, None]
    live_mask = (
        jnp.arange(cache_len, dtype=jnp.int32)[None, None, None, :] < lengths[:, None, None, None]
    )
    remain = jnp.where(live_mask, jax.nn.log_sigmoid(-scores), 0.0)
    after_sum = lax.cumsum(remain, axis=3, reverse=True) - remain
    weights = jnp.where(live_mask, jnp.exp(jax.nn.log_sigmoid(scores) + after_sum), 0.0).astype(
        jnp.bfloat16
    )
    attended = jnp.einsum(
        "bkgl,blkd->bkgd", weights, value_heads, preferred_element_type=jnp.float32
    )
    return attended.reshape(batch_rows, HEADS * HEAD_DIM).astype(jnp.bfloat16)


def plain(
    tokens,
    lengths,
    cache_key,
    cache_value,
    routes,
    route_logits,
    mix_gain,
    query_gain,
    key_gain,
    head_bias,
    w_query,
    w_key,
    w_value,
    w_out,
    ffn_gain,
    w_gate,
    w_up,
    w_down,
):
    token_rows = tokens.shape[0]
    key_width = w_key.shape[1]
    as_float = tokens.astype(jnp.float32)
    normed = rms_scaled(as_float, mix_gain).astype(jnp.bfloat16)
    pieces = (
        lax.all_gather(w_query, "ep", axis=0, tiled=True),
        lax.all_gather(w_key, "ep", axis=0, tiled=True),
        lax.all_gather(w_value, "ep", axis=0, tiled=True),
    )
    queries, fresh_key, fresh_value = tuple(
        (jnp.dot(normed, weight, preferred_element_type=jnp.float32) for weight in pieces)
    )
    new_key = rms_scaled(fresh_key.reshape(token_rows, KV_HEADS, HEAD_DIM), key_gain)
    new_key = new_key.reshape(token_rows, key_width).astype(jnp.bfloat16)
    new_value = fresh_value.astype(jnp.bfloat16)
    attended = stick_attend(queries, lengths, cache_key, cache_value, query_gain, head_bias)
    mixed = as_float + jnp.dot(
        attended,
        lax.all_gather(w_out, "ep", axis=1, tiled=True),
        preferred_element_type=jnp.float32,
    )
    expert_in = rms_scaled(mixed, ffn_gain).astype(jnp.bfloat16)
    every_gate = lax.all_gather(route_weights(routes, route_logits), "ep", axis=0, tiled=True)
    ff_share = w_gate.shape[1]
    my_expert = lax.axis_index("ep") // (FF // ff_share)
    my_gate = lax.dynamic_slice_in_dim(every_gate, my_expert, 1, 1)
    input_rows = lax.all_gather(expert_in, "ep", axis=0, tiled=True)
    gate_value = jnp.dot(input_rows, w_gate, preferred_element_type=jnp.float32)
    up_value = jnp.dot(input_rows, w_up, preferred_element_type=jnp.float32)
    hidden = (jax.nn.silu(gate_value) * up_value * my_gate).astype(jnp.bfloat16)
    expert_sum = lax.psum_scatter(
        jnp.dot(hidden, w_down, preferred_element_type=jnp.float32),
        "ep",
        scatter_dimension=0,
        tiled=True,
    )
    return ((mixed + expert_sum).astype(jnp.bfloat16), new_key, new_value)


WEIGHT_PARTS = 2
PAIR_LAG = 2
DOWN_WIDTHS = (512, 512, 512, 512)
SCHEDULE = (0, (0,), 1, 2, 3, 4, (1,), 5, (2,), 6, (3,), 7, (4,), (5,), (6,), (7,))
COLUMNS = 256


def dot(left, right):
    return jnp.dot(left, right, preferred_element_type=jnp.float32)


def iota(shape, dim):
    return lax.broadcasted_iota(jnp.int32, shape, dim)


def column(row):
    square = (row.shape[1], row.shape[1])
    return jnp.sum(
        jnp.where(iota(square, 0) == iota(square, 1), jnp.broadcast_to(row, square), 0.0),
        axis=1,
        keepdims=True,
    )


def finish(*refs):
    half = len(refs) // 2
    copies = [
        pltpu.make_async_copy(refs[i], refs[half + i], refs[-1].at[i]) for i in range(half)
    ]
    for copy in copies:
        copy.start()
    for copy in copies:
        copy.wait()


def fused(
    n,
    tokens_hbm,
    lengths_hbm,
    ck_hbm,
    cv_hbm,
    routes_hbm,
    logits_hbm,
    mix_gain_hbm,
    query_gain_hbm,
    key_gain_hbm,
    head_bias_hbm,
    wq_hbm,
    wk_hbm,
    wv_hbm,
    wo_hbm,
    ffn_gain_hbm,
    wg_hbm,
    wu_hbm,
    wd_hbm,
    out_any,
    new_key_any,
    new_value_any,
    tokens_ref,
    lengths_ref,
    routes_ref,
    logits_ref,
    mix_gain_ref,
    query_gain_ref,
    key_gain_ref,
    head_bias_ref,
    ffn_gain_ref,
    out_ref,
    new_key_ref,
    new_value_ref,
    wq_raw,
    wqkv,
    wo,
    ck,
    kt,
    cv,
    wg,
    wu,
    wd,
    s1,
    r1,
    s2,
    r2,
    s2kv,
    r2kv,
    s3,
    r3,
    r4,
    s5,
    p5,
    own5,
    t5,
    r5,
    gates_all,
    token_cols,
    aux_rows,
    attended_rows,
    own_mixed,
    gate_acc,
    up_acc,
    hidden,
    operand_sem,
    small_sem,
    send_sem,
    recv_sem,
    direct_sem,
    relay_sem,
    pair_sem,
    spread_sem,
    twin_sem,
):
    me = lax.axis_index("ep")
    core, chip = me % 2, me // 2
    chips = n // 2
    other = 1 - core
    sibling = 2 * chip + other
    rows, width = tokens_ref.shape
    half_rows = rows * chips
    all_rows = rows * n
    share = width // n
    chip_share = width // chips
    q_width, k_width = wq_hbm.shape[1], wk_hbm.shape[1]
    cache_len = ck.shape[1]
    group_size = HEADS // KV_HEADS
    ff_share = wg.shape[1]
    my_expert = me // (FF // ff_share)

    barrier = pltpu.get_barrier_semaphore()
    chip_at = [chip]
    for k in range(1, chips):
        bit = k.bit_length() - 1
        flip = 2**bit * (1 - 2 * ((chip // 2**bit) % 2))
        chip_at.append(chip_at[k - 2**bit] + flip)
    peer_at = [2 * c + other for c in chip_at]
    furthest_first = range(chips - 1, -1, -1)
    for k in furthest_first:
        pl.semaphore_signal(
            barrier,
            inc=1,
            device_id={"ep": peer_at[k]},
            device_id_type=pl.DeviceIdType.MESH,
        )

    operands = [
        pltpu.make_async_copy(a, b, operand_sem.at[i])
        for i, (a, b) in enumerate(
            (
                (tokens_hbm, tokens_ref),
                (routes_hbm, routes_ref),
                (logits_hbm, logits_ref),
                (mix_gain_hbm, mix_gain_ref),
                (query_gain_hbm, query_gain_ref),
                (key_gain_hbm, key_gain_ref),
                (head_bias_hbm, head_bias_ref),
                (ffn_gain_hbm, ffn_gain_ref),
                (lengths_hbm, lengths_ref),
            )
        )
    ]
    for c in operands:
        c.start()

    my_rows = pl.ds(pl.multiple_of(core * share, share), share)
    small = [
        pltpu.make_async_copy(a, b, small_sem.at[i])
        for i, (a, b) in enumerate(
            (
                (wq_hbm, wq_raw),
                (wk_hbm, wqkv.at[my_rows, q_width : q_width + k_width]),
                (wv_hbm, wqkv.at[my_rows, q_width + k_width :]),
            )
        )
    ]
    for head in range(HEADS):
        place = head % group_size * KV_HEADS + head // group_size
        small.append(
            pltpu.make_async_copy(
                wo_hbm.at[head * HEAD_DIM : (head + 1) * HEAD_DIM],
                wo.at[core, place * HEAD_DIM : (place + 1) * HEAD_DIM],
                small_sem.at[3],
            )
        )
    for c in small:
        c.start()
    caches = [pltpu.make_async_copy(ck_hbm.at[b], ck.at[b], operand_sem.at[0]) for b in range(rows)]
    caches += [pltpu.make_async_copy(cv_hbm.at[b], cv.at[b], operand_sem.at[1]) for b in range(rows)]
    weights = []
    for which, (a, b) in enumerate(((wg_hbm, wg), (wu_hbm, wu), (wd_hbm, wd))):
        step = b.shape[0] // WEIGHT_PARTS
        for part in range(WEIGHT_PARTS):
            piece = pl.ds(part * step, step)
            weights.append(pltpu.make_async_copy(a.at[piece], b.at[piece], operand_sem.at[2 + which]))

    results = [
        pltpu.make_async_copy(a, b, operand_sem.at[5 + i])
        for i, (a, b) in enumerate(
            ((out_ref, out_any), (new_key_ref, new_key_any), (new_value_ref, new_value_any))
        )
    ]
    for c in operands:
        c.wait()

    def send(stage, device, source, target, arrival):
        pltpu.make_async_remote_copy(
            src_ref=source,
            dst_ref=target,
            send_sem=send_sem.at[stage],
            recv_sem=arrival,
            device_id={"ep": device},
            device_id_type=pl.DeviceIdType.MESH,
        ).start()

    def arrived(sem, blocks):
        pltpu.make_async_copy(blocks, blocks, sem).wait()

    others = pl.ds(0, chips - 1)

    as_float = tokens_ref[...].astype(jnp.float32)
    scale = lax.rsqrt(jnp.mean(as_float * as_float, axis=1, keepdims=True) + EPSILON)
    lane = iota((rows, 128), 1)
    logit_gap = column(logits_ref[0:1] - logits_ref[1:2])
    chosen = [column(routes_ref[i : i + 1].astype(jnp.float32)) for i in range(2)]
    first_share = 1.0 / (1.0 + jnp.exp(-logit_gap))
    second_share = 1.0 / (1.0 + jnp.exp(logit_gap))
    expert_lane = (lane % EXPERTS).astype(jnp.float32)
    gates = jnp.where(chosen[0] == expert_lane, first_share, 0.0) + jnp.where(
        chosen[1] == expert_lane, second_share, 0.0
    )
    aux = jnp.where(lane < 3 * EXPERTS, gates, scale)
    high = aux.astype(jnp.bfloat16).astype(jnp.float32)
    middle = (aux - high).astype(jnp.bfloat16).astype(jnp.float32)
    low = aux - high - middle
    term = jnp.where(lane < 3 * EXPERTS, lane // EXPERTS, lane - 3 * EXPERTS)
    aux = jnp.where(term == 0, high, jnp.where(term == 1, middle, low))
    aux = jnp.concatenate([aux] * (chip_share // 128), axis=1)
    for p in range(chips):
        s1[p] = jnp.concatenate(
            [as_float[:, p * chip_share : (p + 1) * chip_share], aux], axis=0
        ).astype(jnp.bfloat16)
    for c in small[:3]:
        c.wait()
    left_half = iota((share, 2 * HEAD_DIM), 1) < HEAD_DIM
    for place in range(0, HEADS, 2):
        halves = []
        for side in range(2):
            head = (place + side) % KV_HEADS * group_size + (place + side) // KV_HEADS
            start = head // 2 * 2 * HEAD_DIM
            half = wq_raw[:, start : start + 2 * HEAD_DIM].astype(jnp.float32)
            halves.append(half if head % 2 == side else pltpu.roll(half, HEAD_DIM, 1))
        wqkv[my_rows, place * HEAD_DIM : (place + 2) * HEAD_DIM] = jnp.where(
            left_half, halves[0], halves[1]
        ).astype(jnp.bfloat16)
    pl.semaphore_wait(barrier, chips)
    for k in furthest_first:
        send(0, peer_at[k], s1.at[chip_at[k]], r1.at[chip], recv_sem.at[0])
    query_half = wqkv.at[my_rows, 0:q_width]
    send(4, sibling, query_half, query_half, twin_sem.at[0])
    for c in caches:
        c.start()
    arrived(recv_sem.at[0], r1)
    for c in weights:
        c.start()
    for p in range(chips):
        block = r1[p].astype(jnp.float32)
        token_cols[p * rows : (p + 1) * rows, :] = block[:rows]
        aux_rows[p * rows : (p + 1) * rows, :] = block[rows:, :128]
    aux = aux_rows[...]
    lane = iota(aux.shape, 1)
    row_scale = jnp.sum(
        jnp.where((lane >= 3 * EXPERTS) & (lane < 3 * EXPERTS + 3), aux, 0.0), axis=1, keepdims=True
    )
    my_gain = mix_gain_ref[:, pl.ds(pl.multiple_of(chip * chip_share, chip_share), chip_share)]
    normed = (token_cols[...] * row_scale * my_gain).astype(jnp.bfloat16)
    arrived(twin_sem.at[0], query_half)

    partial = dot(normed, wqkv[:, :q_width])
    for p in range(chips):
        s2[p] = partial[p * rows : (p + 1) * rows].astype(jnp.bfloat16)
    for k in furthest_first:
        send(1, peer_at[k], s2.at[chip_at[k]], r2.at[chip], recv_sem.at[1])
    key_value_half = wqkv.at[my_rows, q_width:]
    send(3, sibling, key_value_half, key_value_half, twin_sem.at[3])
    my_gate = jnp.sum(
        jnp.where((lane < 3 * EXPERTS) & (lane % EXPERTS == my_expert), aux, 0.0),
        axis=1,
        keepdims=True,
    )
    gates_all[other] = jnp.broadcast_to(my_gate, aux.shape)
    send(5, sibling, gates_all.at[other], gates_all.at[other], twin_sem.at[2])

    own_group = iota((HEADS, k_width), 1) // HEAD_DIM == iota((HEADS, k_width), 0) % KV_HEADS
    later = jnp.where(
        iota((COLUMNS, COLUMNS), 0) > iota((COLUMNS, COLUMNS), 1), 1.0, 0.0
    ).astype(jnp.bfloat16)
    query_gain = jnp.concatenate([query_gain_ref[...]] * KV_HEADS, axis=1)
    key_gain = jnp.concatenate([key_gain_ref[...]] * KV_HEADS, axis=1)
    blocks = cache_len // COLUMNS
    head_rows = rows * HEADS
    place, head = iota((HEADS, HEADS), 0), iota((HEADS, HEADS), 1)
    head_bias = jnp.where(
        head == place % KV_HEADS * group_size + place // KV_HEADS,
        jnp.broadcast_to(head_bias_ref[...], head.shape),
        0.0,
    )
    head_bias = jnp.concatenate([jnp.sum(head_bias, axis=1, keepdims=True)] * rows, axis=0)
    out_row, in_row = iota((group_size * rows, head_rows), 0), iota((group_size * rows, head_rows), 1)
    gather = jnp.where(
        (out_row % rows == in_row // HEADS) & (out_row // rows == in_row % HEADS // KV_HEADS),
        1.0,
        0.0,
    ).astype(jnp.bfloat16)
    row_of = iota((head_rows, 1), 0) // HEADS
    lengths = jnp.zeros((head_rows, 1), jnp.int32)
    for b in range(rows):
        lengths = jnp.where(row_of == b, lengths_ref[:, b : b + 1], lengths)
    live = iota((head_rows, cache_len), 1) < lengths
    arrived(operand_sem.at[0], ck)
    for b in range(rows):
        kt[b] = ck[b].T
    arrived(operand_sem.at[1], cv)

    arrived(twin_sem.at[3], key_value_half)
    partial = dot(normed, wqkv[:, q_width:])
    for p in range(chips):
        s2kv[p] = partial[p * rows : (p + 1) * rows].astype(jnp.bfloat16)
    arrived(recv_sem.at[1], r2)
    for k in furthest_first:
        send(2, peer_at[k], s2kv.at[chip_at[k]], r2kv.at[chip], recv_sem.at[3])
    arrived(small_sem.at[3], wo.at[core])
    arrived(send_sem.at[4], query_half)
    send(4, sibling, wo.at[core], wo.at[core], twin_sem.at[1])
    total = r2[0].astype(jnp.float32)
    for p in range(1, chips):
        total = total + r2[p].astype(jnp.float32)
    queries = total
    spread = []
    for b in range(rows):
        wide = [
            jnp.broadcast_to(
                queries[b : b + 1, i * k_width : (i + 1) * k_width], (KV_HEADS, k_width)
            )
            for i in range(group_size)
        ]
        wide = jnp.where(own_group, jnp.concatenate(wide, axis=0), 0.0)
        mean = jnp.sum(wide * wide, axis=1, keepdims=True) / HEAD_DIM
        spread.append((wide * lax.rsqrt(mean + EPSILON) * query_gain).astype(jnp.bfloat16))
    scores = jnp.concatenate([dot(spread[b], kt[b]) for b in range(rows)], axis=0)
    scores = scores * HEAD_DIM ** (-0.5) + head_bias
    tail_log = jnp.log(1.0 + jnp.exp(-jnp.abs(scores)))
    remain = jnp.where(live, jnp.minimum(-scores, 0.0) - tail_log, 0.0)
    pieces = [remain[:, i * COLUMNS : (i + 1) * COLUMNS] for i in range(blocks)]
    highs = [block.astype(jnp.bfloat16) for block in pieces]
    lows = [
        (block - high.astype(jnp.float32)).astype(jnp.bfloat16)
        for block, high in zip(pieces, highs)
    ]
    sums = dot(jnp.concatenate(highs + lows, axis=0), later)
    after = [None] * blocks
    carry = jnp.zeros((head_rows, 1), jnp.float32)
    for i in reversed(range(blocks)):
        low = (blocks + i) * head_rows
        after[i] = (
            sums[i * head_rows : (i + 1) * head_rows] + sums[low : low + head_rows] + carry
        )
        carry = carry + jnp.sum(pieces[i], axis=1, keepdims=True)
    after_sum = jnp.concatenate(after, axis=1)
    chance = jnp.exp(jnp.minimum(scores, 0.0) - tail_log + after_sum)
    weight = jnp.where(live, chance, 0.0).astype(jnp.bfloat16)
    mixed_heads = jnp.concatenate(
        [dot(weight[b * HEADS : (b + 1) * HEADS], cv[b]) for b in range(rows)], axis=0
    )
    own_groups = jnp.concatenate([own_group] * rows, axis=0)
    heads = jnp.where(own_groups, mixed_heads, 0.0).astype(jnp.bfloat16)
    s3[...] = dot(gather, heads).astype(jnp.bfloat16)

    arrived(send_sem.at[0], s1)
    for k in furthest_first:
        send(0, peer_at[k], s3, r3.at[chip], recv_sem.at[2])

    arrived(twin_sem.at[1], wo.at[core])
    arrived(twin_sem.at[2], gates_all.at[core])

    arrived(recv_sem.at[2], r3)
    for p in range(chips):
        block = r3[p].astype(jnp.float32)
        for i in range(group_size):
            attended_rows[p * rows : (p + 1) * rows, i * k_width : (i + 1) * k_width] = block[
                i * rows : (i + 1) * rows
            ]
    attended_all = attended_rows[...].astype(jnp.bfloat16)
    for h in range(2):
        columns = slice(h * share, (h + 1) * share)
        mixed = token_cols[:, columns] + dot(attended_all, wo[h])
        r4[chip, other, :, columns] = mixed.astype(jnp.bfloat16)

    mine = r4.at[chip, other]
    arrived(send_sem.at[1], s2)
    arrived(send_sem.at[5], gates_all.at[other])
    for k in range(chips):
        send(1, peer_at[k], mine, mine, direct_sem.at[k])
    pick = jnp.where(
        iota((8, half_rows), 1) == iota((8, half_rows), 0) + chip * rows, 1.0, 0.0
    ).astype(jnp.bfloat16)
    squares = jnp.zeros((all_rows, chip_share), jnp.float32)
    gate_column = gates_all[...].reshape(all_rows, 128)[:, :1]
    for which, b in enumerate((wg, wu)):
        arrived(operand_sem.at[2 + which], b)
    arrived(operand_sem.at[4], wd)

    def chunks_of(group, squares, first, last):
        entries = []
        for k in group:
            source = chip_at[k]
            columns = pl.ds(pl.multiple_of(source * chip_share, chip_share), chip_share)
            if k:
                arrived(relay_sem.at[k - 1], r4.at[source, other])
            own_mixed[:, columns] = dot(pick, r4[source, core])[:rows]
            block = r4[source].reshape(all_rows, chip_share).astype(jnp.float32)
            squares = squares + block * block
            entries.append((columns, (block * ffn_gain_ref[:, columns]).astype(jnp.bfloat16)))
        if last:
            scale = lax.rsqrt(jnp.sum(squares, axis=1, keepdims=True) / width + EPSILON)
        for i in range(ff_share // COLUMNS):
            inner = slice(i * COLUMNS, (i + 1) * COLUMNS)
            gate_value = sum(dot(entry, wg[columns, inner]) for columns, entry in entries)
            up_value = sum(dot(entry, wu[columns, inner]) for columns, entry in entries)
            if not first:
                gate_value = gate_value + gate_acc[:, inner]
                up_value = up_value + up_acc[:, inner]
            if last:
                gate_value = gate_value * scale
                silu = gate_value / (1.0 + jnp.exp(-gate_value))
                hidden[:, inner] = (silu * (up_value * scale) * gate_column).astype(jnp.bfloat16)
            else:
                gate_acc[:, inner] = gate_value
                up_acc[:, inner] = up_value
        return squares

    def finish_key_value():
        arrived(recv_sem.at[3], r2kv)
        total = r2kv[0].astype(jnp.float32)
        for p in range(1, chips):
            total = total + r2kv[p].astype(jnp.float32)
        fresh_key = total[:, :k_width]
        new_value_ref[...] = total[:, k_width:].astype(jnp.bfloat16)
        key_squares = fresh_key * fresh_key
        key_lane = iota(key_squares.shape, 1) // HEAD_DIM
        key_scale = jnp.zeros_like(key_squares)
        for g in range(KV_HEADS):
            mean = jnp.sum(jnp.where(key_lane == g, key_squares, 0.0), axis=1, keepdims=True) / HEAD_DIM
            key_scale = jnp.where(key_lane == g, lax.rsqrt(mean + EPSILON), key_scale)
        new_key_ref[...] = (fresh_key * key_scale * key_gain).astype(jnp.bfloat16)
        for c in results[1:]:
            c.start()

    for i, step in enumerate(SCHEDULE):
        if i == 2:
            finish_key_value()
        if isinstance(step, int):
            block = r4.at[chip_at[step], core]
            arrived(direct_sem.at[step], block)
            if step:
                send(6, sibling, block, block, relay_sem.at[step - 1])
        else:
            squares = chunks_of(step, squares, step[0] == 0, i == len(SCHEDULE) - 1)

    parts = len(DOWN_WIDTHS)
    starts = [sum(DOWN_WIDTHS[:part]) for part in range(parts)]

    def spread_sums(part):
        lanes = pl.ds(0, DOWN_WIDTHS[part])
        arrived(pair_sem.at[part], p5.at[part, :, lanes])
        both = own5[part, :, lanes] + p5[part, :, lanes].astype(jnp.float32)
        for p in range(chips):
            t5[part, p, :, lanes] = both[p * rows : (p + 1) * rows].astype(jnp.bfloat16)
        for k in range(chips):
            send(
                7,
                peer_at[k],
                t5.at[part, chip_at[k], :, lanes],
                r5.at[part, chip, :, lanes],
                spread_sem.at[part],
            )

    def down_product(start, lanes):
        return jnp.concatenate(
            [
                dot(hidden[...], wd[:, start + i : start + i + COLUMNS])
                for i in range(0, lanes, COLUMNS)
            ],
            axis=1,
        )

    for part in range(parts):
        lanes = pl.ds(0, DOWN_WIDTHS[part])
        partial = down_product(starts[part], DOWN_WIDTHS[part])
        lower, upper = partial[:half_rows], partial[half_rows:]
        own5[part, :, lanes] = jnp.where(core == 0, upper, lower)
        s5[part, :, lanes] = jnp.where(core == 0, lower, upper).astype(jnp.bfloat16)
        send(5, sibling, s5.at[part, :, lanes], p5.at[part, :, lanes], pair_sem.at[part])
        if part >= PAIR_LAG:
            spread_sums(part - PAIR_LAG)
    for part in range(parts - PAIR_LAG, parts):
        spread_sums(part)
    for part in range(parts):
        lanes = pl.ds(0, DOWN_WIDTHS[part])
        columns = slice(starts[part], starts[part] + DOWN_WIDTHS[part])
        arrived(spread_sem.at[part], r5.at[part, :, :, lanes])
        total = own_mixed[:, columns]
        for p in range(chips):
            total = total + r5[part, p, :, lanes].astype(jnp.float32)
        out_ref[:, columns] = total.astype(jnp.bfloat16)
    results[0].start()
    arrived(send_sem.at[2], s2kv)
    arrived(send_sem.at[3], key_value_half)
    arrived(send_sem.at[0], r3)
    arrived(send_sem.at[1], r4.at[:, 0])
    arrived(send_sem.at[4], wo.at[core])
    arrived(send_sem.at[6], r4.at[others, 0])
    whole = pl.ds(0, width // s5.shape[2])
    arrived(send_sem.at[5], s5.at[whole])
    arrived(send_sem.at[7], t5.at[whole])
    for c in results:
        c.wait()


def local(
    n,
    tokens,
    lengths,
    cache_key,
    cache_value,
    routes,
    route_logits,
    mix_gain,
    query_gain,
    key_gain,
    head_bias,
    w_query,
    w_key,
    w_value,
    w_out,
    ffn_gain,
    w_gate,
    w_up,
    w_down,
):
    rows, width = tokens.shape
    chips = n // 2
    all_rows, half_rows = rows * n, rows * chips
    share, chip_share = width // n, width // chips
    q_width, k_width = w_query.shape[1], w_key.shape[1]
    wide = q_width + k_width + w_value.shape[1]
    parts, step = len(DOWN_WIDTHS), max(DOWN_WIDTHS)
    ff_share = w_gate.shape[1]
    anywhere = pl.BlockSpec(memory_space=pl.ANY)
    bf16, f32 = jnp.bfloat16, jnp.float32

    def like(array):
        return pltpu.VMEM(array.shape, array.dtype)

    flops = 2 * all_rows * 3 * w_gate.shape[0] * w_gate.shape[1]
    shapes = ((rows, width), (rows, k_width), (rows, w_value.shape[1]))
    results = pl.pallas_call(
        functools.partial(fused, n),
        out_shape=tuple(pltpu.VMEM(shape, bf16) for shape in shapes),
        in_specs=[anywhere] * 18,
        out_specs=(anywhere,) * 3,
        scratch_shapes=[
            like(tokens),
            pltpu.VMEM((1, rows), lengths.dtype),
            pltpu.VMEM(routes.shape[::-1], routes.dtype),
            pltpu.VMEM(route_logits.shape[::-1], f32),
            pltpu.VMEM((1, width), f32),
            pltpu.VMEM((1, HEAD_DIM), f32),
            pltpu.VMEM((1, HEAD_DIM), f32),
            pltpu.VMEM((1, HEADS), f32),
            pltpu.VMEM((1, width), f32),
            *(pltpu.VMEM(shape, bf16) for shape in shapes),
            like(w_query),
            pltpu.VMEM((chip_share, wide), bf16),
            pltpu.VMEM((2, *w_out.shape), bf16),
            like(cache_key),
            pltpu.VMEM((rows, k_width, cache_key.shape[1]), bf16),
            like(cache_value),
            like(w_gate),
            like(w_up),
            like(w_down),
            pltpu.VMEM((chips, 2 * rows, chip_share), bf16),
            pltpu.VMEM((chips, 2 * rows, chip_share), bf16),
            pltpu.VMEM((chips, rows, q_width), bf16),
            pltpu.VMEM((chips, rows, q_width), bf16),
            pltpu.VMEM((chips, rows, wide - q_width), bf16),
            pltpu.VMEM((chips, rows, wide - q_width), bf16),
            pltpu.VMEM((rows * q_width // k_width, k_width), bf16),
            pltpu.VMEM((chips, rows * q_width // k_width, k_width), bf16),
            pltpu.VMEM((chips, 2, half_rows, chip_share), bf16),
            pltpu.VMEM((parts, half_rows, step), bf16),
            pltpu.VMEM((parts, half_rows, step), bf16),
            pltpu.VMEM((parts, half_rows, step), f32),
            pltpu.VMEM((parts, chips, rows, step), bf16),
            pltpu.VMEM((parts, chips, rows, step), bf16),
            pltpu.VMEM((2, half_rows, 128), f32),
            pltpu.VMEM((half_rows, chip_share), f32),
            pltpu.VMEM((half_rows, 128), f32),
            pltpu.VMEM((half_rows, q_width), f32),
            pltpu.VMEM((rows, width), f32),
            pltpu.VMEM((all_rows, ff_share), f32),
            pltpu.VMEM((all_rows, ff_share), f32),
            pltpu.VMEM((all_rows, ff_share), bf16),
            pltpu.SemaphoreType.DMA((9,)),
            pltpu.SemaphoreType.DMA((4,)),
            pltpu.SemaphoreType.DMA((8,)),
            pltpu.SemaphoreType.DMA((4,)),
            pltpu.SemaphoreType.DMA((chips,)),
            pltpu.SemaphoreType.DMA((chips - 1,)),
            pltpu.SemaphoreType.DMA((parts,)),
            pltpu.SemaphoreType.DMA((parts,)),
            pltpu.SemaphoreType.DMA((4,)),
        ],
        compiler_params=pltpu.CompilerParams(
            collective_id=0, has_side_effects=True, vmem_limit_bytes=60 * 1024 * 1024
        ),
        cost_estimate=pl.CostEstimate(flops=flops, bytes_accessed=flops // all_rows, transcendentals=0),
    )(
        tokens,
        lengths.reshape(1, -1),
        cache_key,
        cache_value,
        routes.T,
        route_logits.T,
        mix_gain.reshape(1, -1),
        query_gain.reshape(1, -1),
        key_gain.reshape(1, -1),
        head_bias.reshape(1, -1),
        w_query,
        w_key,
        w_value,
        w_out,
        ffn_gain.reshape(1, -1),
        w_gate,
        w_up,
        w_down,
    )
    return pl.pallas_call(
        finish,
        out_shape=tuple(jax.ShapeDtypeStruct(shape, bf16) for shape in shapes),
        in_specs=[anywhere] * len(shapes),
        out_specs=(anywhere,) * len(shapes),
        scratch_shapes=[pltpu.SemaphoreType.DMA((len(shapes),))],
    )(*(pltpu.with_memory_space_constraint(result, pltpu.VMEM) for result in results))


def solution(mesh):
    n = mesh.shape["ep"]

    def body(*arrays):
        tokens, w_gate = arrays[0], arrays[15]
        share = tokens.shape[1] // n
        aligned = share == 128 and n & (n - 1) == 0 and n % 4 == 0
        halves = (FF // w_gate.shape[1]) % 2 == 0 and arrays[13].shape[1] == share
        if aligned and halves and w_gate.shape[1] % COLUMNS == 0 and tokens.shape[0] * n % 64 == 0 and tokens.shape[1] == sum(DOWN_WIDTHS):
            return local(n, *arrays)
        return plain(*arrays)

    return jax.shard_map(
        body,
        mesh=mesh,
        in_specs=(
            P(("grp", "ep"), None),
            P(("grp", "ep")),
            P(("grp", "ep"), None, None),
            P(("grp", "ep"), None, None),
            P(("grp", "ep"), None),
            P(("grp", "ep"), None),
            P(),
            P(),
            P(),
            P(),
            P("ep", None),
            P("ep", None),
            P("ep", None),
            P(None, "ep"),
            P(),
            P(None, "ep"),
            P(None, "ep"),
            P("ep", None),
        ),
        out_specs=(P(("grp", "ep"), None), P(("grp", "ep"), None), P(("grp", "ep"), None)),
        check_vma=False,
    )
```
